128 devices in a mesh: kv: 16 (over z, y), tp: 8 (over x, core).
Axes of the slice: x: 4, y: 4, z: 4, core: 2. Of those that a mesh axis runs over, the one named last changes fastest.
Arguments:
- tokens: bfloat16 [4096, 4096], P('kv'), may hold values from -6 to 6
- norm_gain: float32 [4096], replicated, may hold values from 0.1 to 1.9
- w_query: bfloat16 [4096, 2048], P('kv', 'tp'), may hold values from -0.09375 to 0.09375
- w_forget: bfloat16 [4096, 2048], P('kv', 'tp'), may hold values from -0.09375 to 0.09375
- w_value: bfloat16 [4096, 2048], P('kv', 'tp'), may hold values from -0.09375 to 0.09375
- w_gate: bfloat16 [4096, 2048], P('kv', 'tp'), may hold values from -0.09375 to 0.09375
- lower_bound: float32 [2048], P('tp'), may hold values from 0 to 0.9
- head_gain: float32 [2048], P('tp'), may hold values from 0.1 to 1.9
- w_out: bfloat16 [2048, 4096], P('kv', 'tp'), may hold values from -0.125 to 0.125
- state: float32 [1024, 16, 128, 128], P('kv', 'tp'), may hold values from -4 to 4
- prev_forget: bfloat16 [1024, 4, 2048], P('kv', None, 'tp'), may hold values from -8 to 8
- prev_value: bfloat16 [1024, 4, 2048], P('kv', None, 'tp'), may hold values from -6 to 6
- accepted: int32 [1024], P('kv'), may hold values from 0 to 4
Outputs:
- mixed: bfloat16 [4096, 4096], P('kv', 'tp')
- taken_state: float32 [1024, 16, 128, 128], P('kv', 'tp')
The draws below stay inside these ranges and needn't reach their ends.
All inputs are finite; a program needn't handle non-finite values.
Results may differ from the reference program's by a relative error of at most 0.015.
Values may be sent and summed in bfloat16 or wider, within the bound.
A program may use at most 128 MiB of HBM per device.

```python
import jax
import jax.numpy as jnp
from jax import lax

D = 4096
HEADS = 16
KEY_DIM = 128
VAL_DIM = 128
PROPOSALS = 4
SEQS = 1024
TOKENS = 4096
WIDTH = 2048


def with_ends(entries, own_key, least, largest):
    longest = entries.shape.index(max(entries.shape))
    spots = []
    for shift in (0, 1):
        where = [jax.random.randint(jax.random.fold_in(own_key, axis), (), 0, length) for axis, length in enumerate(entries.shape)]
        where[longest] = (where[longest] + shift) % entries.shape[longest]
        spots.append(tuple(where))
    return entries.at[spots[0]].set(least).at[spots[1]].set(largest)


def steps_of(own_key, extent, split, smallest, top_value):
    loudness, own = 1.0, jax.random.fold_in(own_key, 6)
    for axis_at, shards_of in split:
        heights = jnp.exp(jax.random.uniform(jax.random.fold_in(own, axis_at), (shards_of,), jnp.float32, smallest / len(split), top_value / len(split)))
        loudness = loudness * jnp.repeat(heights, extent[axis_at] // shards_of).reshape([-1 if axis == axis_at else 1 for axis in range(len(extent))])
    return loudness


def bell_draw(key, shape, width, reach, shards=(), kind=jnp.bfloat16):
    loudness = steps_of(key, shape, shards, -0.22, 0.18) if shards else 1.0
    result = jax.random.normal(key, shape, jnp.float32) * width * loudness
    return jnp.minimum(jnp.maximum(result, -reach), reach).astype(kind)


def setup_inputs(seed: int = 0) -> dict:
    key_of = jax.random.split(jax.random.key(seed), 14)
    return {
        "tokens": bell_draw(key_of[0], (TOKENS, D), 1.0, 6.0, ((0, 16),)),
        "norm_gain": jnp.clip(1.0 + 0.18 * jax.random.normal(key_of[1], (D,), jnp.float32), 0.1, 1.9),
        "w_query": bell_draw(key_of[2], (D, WIDTH), D ** -0.5, 0.09375, ((0, 16), (1, 8))),
        "w_forget": bell_draw(key_of[3], (D, WIDTH), D ** -0.5, 0.09375, ((0, 16), (1, 8))),
        "w_value": bell_draw(key_of[4], (D, WIDTH), D ** -0.5, 0.09375, ((0, 16), (1, 8))),
        "w_gate": bell_draw(key_of[5], (D, WIDTH), D ** -0.5, 0.09375, ((0, 16), (1, 8))),
        "lower_bound": jnp.clip(0.9 * jax.random.uniform(key_of[6], (WIDTH,), jnp.float32) ** steps_of(key_of[6], (WIDTH,), ((0, 8),), -0.2, 0.2), 0.0, 0.9),
        "head_gain": jnp.clip(1.0 + 0.18 * jax.random.normal(key_of[7], (WIDTH,), jnp.float32), 0.1, 1.9),
        "w_out": bell_draw(key_of[8], (WIDTH, D), WIDTH ** -0.5, 0.125, ((0, 16), (1, 8))),
        "state": bell_draw(key_of[9], (SEQS, HEADS, KEY_DIM, VAL_DIM), 0.5, 4.0, ((0, 16), (1, 8)), jnp.float32),
        "prev_forget": bell_draw(key_of[10], (SEQS, PROPOSALS, WIDTH), 1.5, 8.0, ((0, 16), (2, 8))),
        "prev_value": bell_draw(key_of[11], (SEQS, PROPOSALS, WIDTH), 1.0, 6.0, ((0, 16), (2, 8))),
        "accepted": with_ends(jax.random.randint(key_of[12], (SEQS,), 0, PROPOSALS + 1), jax.random.fold_in(key_of[12], 1), 0, PROPOSALS).astype(jnp.int32),
    }


EPSILON = 1e-06

def forget_of(pre_act, bounds):
    return bounds + (1.0 - bounds) * jax.nn.sigmoid(pre_act.astype(jnp.float32))

def recur_one(start_state, old_forget, old_values, accepted_count, queries, forget, new_values):
    carried = start_state
    for position in range(old_forget.shape[0]):
        kept_mask = position < accepted_count
        decay_rate = jnp.where(kept_mask, old_forget[position], 1.0)
        weight = jnp.where(kept_mask, 1.0 - old_forget[position], 0.0)
        carried = decay_rate[:, :, None] * carried + weight[:, :, None] * old_values[position][:, None, :]
    taken = carried
    outputs = []
    for position in range(queries.shape[0]):
        carried = forget[position][:, :, None] * carried + (1.0 - forget[position])[:, :, None] * new_values[position][:, None, :]
        outputs.append(jnp.einsum('hd,hde->he', queries[position], carried, precision=lax.Precision.HIGHEST))
    return (taken, jnp.stack(outputs))

def finish(outputs, head_gain, gate_proj):
    scaled = outputs * lax.rsqrt(lax.optimization_barrier(jnp.mean(outputs * outputs, axis=-1, keepdims=True)) + EPSILON)
    flat = scaled.reshape(gate_proj.shape)
    return (flat * head_gain * jax.nn.silu(gate_proj.astype(jnp.float32))).astype(jnp.bfloat16)

def reference(tokens, norm_gain, w_query, w_forget, w_value, w_gate, lower_bound, head_gain, w_out, state, prev_forget, prev_value, accepted):
    floated = tokens.astype(jnp.float32)
    normed = (floated * lax.rsqrt(lax.optimization_barrier(jnp.mean(floated * floated, axis=-1, keepdims=True)) + EPSILON) * norm_gain).astype(jnp.bfloat16)
    query_proj = jnp.dot(normed, w_query, preferred_element_type=jnp.float32).astype(jnp.bfloat16)
    forget_proj = jnp.dot(normed, w_forget, preferred_element_type=jnp.float32).astype(jnp.bfloat16)
    value_proj = jnp.dot(normed, w_value, preferred_element_type=jnp.float32).astype(jnp.bfloat16)
    gate_proj = jnp.dot(normed, w_gate, preferred_element_type=jnp.float32).astype(jnp.bfloat16)
    seq_total = state.shape[0]
    bounds = lower_bound.reshape(HEADS, KEY_DIM)
    queries = query_proj.astype(jnp.float32).reshape(seq_total, PROPOSALS, HEADS, KEY_DIM) * KEY_DIM ** (-0.5)
    forget = forget_of(forget_proj.reshape(seq_total, PROPOSALS, HEADS, KEY_DIM), bounds)
    new_values = value_proj.astype(jnp.float32).reshape(seq_total, PROPOSALS, HEADS, VAL_DIM)
    old_forget = forget_of(prev_forget.reshape(seq_total, PROPOSALS, HEADS, KEY_DIM), bounds)
    old_values = prev_value.astype(jnp.float32).reshape(seq_total, PROPOSALS, HEADS, VAL_DIM)
    taken, outputs = lax.map(lambda packed: recur_one(*packed), (state, old_forget, old_values, accepted, queries, forget, new_values))
    head_out = finish(outputs, head_gain, gate_proj)
    mixed = jnp.dot(head_out, w_out, preferred_element_type=jnp.float32).astype(jnp.bfloat16)
    return (mixed, taken)
```

```python
import functools
import heapq

import jax
import jax.numpy as jnp
from jax import lax
from jax.experimental import pallas as pl
from jax.experimental.pallas import tpu as pltpu
from jax.sharding import Mesh
from jax.sharding import PartitionSpec as P

EPSILON = 1e-06
MESH = pl.DeviceIdType.MESH
F32, BF16 = jnp.float32, jnp.bfloat16

FIRST = ("y", "y", "z", "z")
SIGN = (1, -1, 1, -1)
OTHER = {"y": "z", "z": "y"}


def forwards(u, a, b):
    first, second, sign = FIRST[u], OTHER[FIRST[u]], SIGN[u]
    if b == 0:
        go = [(second, sign), (second, -sign)]
        if a == 0:
            return [(first, sign), (first, -sign)] + go
        if a == (-sign) % 4:
            return [(first, sign)] + go
        return go
    return [(second, sign)] if b == (-sign) % 4 else []


def lands_at(u, a, b, axis, way):
    if axis == FIRST[u]:
        return (a - way) % 4, b
    return a, (b - way) % 4


@functools.cache
def arrival_order(wire=2.8, delay=2.0):
    free, events, count = {}, [], 0

    def send(now, u, a, b, axis, way):
        nonlocal count
        end = max(now, free.get((axis, way), 0.0)) + wire
        free[axis, way] = end
        count += 1
        heapq.heappush(events, (end + delay, count, u, *lands_at(u, a, b, axis, way)))

    own = [(u, *go) for u in range(4) for go in forwards(u, 0, 0)]
    own.sort(key=lambda item: item[1] != FIRST[item[0]])
    for u, axis, way in own:
        send(0.0, u, 0, 0, axis, way)
    order = []
    while events:
        now, _, u, a, b = heapq.heappop(events)
        order.append((u, a, b))
        for axis, way in forwards(u, a, b):
            send(now, u, a, b, axis, way)
    return tuple(own), tuple(order)


def spot(u, a, b):
    return u * 16 + a * 4 + b


def gate_of(pre_act, bound):
    return bound + (1.0 - bound) * jax.nn.sigmoid(pre_act)


def taken_kernel(forget_ref, value_ref, bound_ref, accepted_ref, state_ref, taken_ref):
    seqs = state_ref.shape[0]
    count = accepted_ref[...]
    bound = bound_ref[...]
    gates, keys = [], []
    for t in range(4):
        kept = t < count
        g = gate_of(forget_ref[:, t, :].astype(F32), bound)
        gates.append(jnp.where(kept, g, 1.0))
        keys.append(jnp.where(kept, 1.0 - g, 0.0))
    after = jnp.ones_like(gates[0])
    weights = [None] * 4
    for t in (3, 2, 1, 0):
        weights[t] = keys[t] * after
        after = after * gates[t]

    def two_parts(x):
        high = x.astype(BF16).astype(F32)
        return high, x - high

    parts = [two_parts(w) for w in weights]
    whole = two_parts(after)
    rows = [p[0] for p in parts] + [p[1] for p in parts] + [whole[0], whole[1]]
    left = jnp.concatenate(rows, axis=0)
    values = jnp.concatenate([value_ref[:, t, :].astype(F32) for t in range(4)] * 2, axis=0)
    height = 10 * seqs
    values = jnp.concatenate([values, jnp.zeros((2 * seqs, values.shape[1]), F32)], axis=0)
    row = lax.broadcasted_iota(jnp.int32, (height, 128), 0)
    for h in range(2):
        lanes = slice(128 * h, 128 * h + 128)
        v = values[:, lanes]
        right = []
        for j in range(seqs):
            mine = row % seqs == j
            right.append(jnp.where(mine, v, 0.0))
            right.append(jnp.where(mine & (row >= 8 * seqs), 1.0, 0.0))
        right = jnp.concatenate(right, axis=1).astype(BF16)
        both = lax.dot_general(
            left[:, lanes].astype(BF16), right, (((0,), (0,)), ((), ())), preferred_element_type=F32
        )
        for j in range(seqs):
            added = both[:, 256 * j : 256 * j + 128]
            decay = both[:, 256 * j + 128 : 256 * j + 256]
            taken_ref[j, h] = state_ref[j, h] * decay + added


def taken_of(prev_forget, prev_value, lower_bound, accepted, state):
    seqs, per = state.shape[0], 8
    return pl.pallas_call(
        taken_kernel,
        grid=(seqs // per,),
        in_specs=[
            pl.BlockSpec((per, 4, 256), lambda i: (i, 0, 0)),
            pl.BlockSpec((per, 4, 256), lambda i: (i, 0, 0)),
            pl.BlockSpec((1, 256), lambda i: (0, 0)),
            pl.BlockSpec((per, 1), lambda i: (i, 0)),
            pl.BlockSpec((per, 2, 128, 128), lambda i: (i, 0, 0, 0)),
        ],
        out_specs=pl.BlockSpec((per, 2, 128, 128), lambda i: (i, 0, 0, 0)),
        out_shape=jax.ShapeDtypeStruct(state.shape, F32),
        name="taken_state",
    )(prev_forget, prev_value, lower_bound.reshape(1, 256), accepted.reshape(seqs, 1), state)


def layer_kernel(
    tokens, gain, w0, w1, w2, w3, bound, head_gain, w_out, taken,
    mixed,
    raw, normed, gathered, sums, out_weights, halves, packed, heads, queries, rest,
    send_sem, wide_recv, out_recv, out_send, head_send, head_recv, relay_recv, local_sem, state_sem,
):
    z, y, x, c = (lax.axis_index(name) for name in ("z", "y", "x", "c"))
    here = {"z": z, "y": y}
    mine = z * 4 + y
    me = x * 2 + c
    weights = (w0, w1, w2, w3)

    barrier = pltpu.get_barrier_semaphore()
    partners = [{axis: (here[axis] + way) % 4} for axis in ("y", "z") for way in (1, 3)]
    partners += [{"x": (x + way) % 4} for way in (1, 2, 3)] + [{"c": 1 - c}]
    for partner in partners:
        pl.semaphore_signal(barrier, inc=1, device_id=partner, device_id_type=MESH)

    token_copy = pltpu.make_async_copy(tokens, raw, local_sem.at[0])
    token_copy.start()
    own_copies = [
        pltpu.make_async_copy(weights[u], gathered.at[u, mine], local_sem.at[1 + u]) for u in range(4)
    ]
    own_copies.append(pltpu.make_async_copy(w_out, out_weights.at[mine], local_sem.at[5]))
    for copy in own_copies:
        copy.start()

    def state_copy(i):
        return pltpu.make_async_copy(
            taken.at[pl.ds(8 * i, 8)], halves.at[i % 2], state_sem.at[i % 2]
        )

    state_copy(0).start()
    state_copy(1).start()
    pl.semaphore_wait(barrier, len(partners))

    def owner(u, a, b):
        at = {FIRST[u]: a, OTHER[FIRST[u]]: b}
        return (z + at["z"]) % 4 * 4 + (y + at["y"]) % 4

    def wide(u, a, b, axis, way):
        k = owner(u, a, b)
        return pltpu.make_async_remote_copy(
            src_ref=weights[u] if a == b == 0 else gathered.at[u, k],
            dst_ref=gathered.at[u, k],
            send_sem=send_sem,
            recv_sem=wide_recv.at[spot(u, *lands_at(u, a, b, axis, way))],
            device_id={axis: (here[axis] + way) % 4},
            device_id_type=MESH,
        )

    def wide_arrival(u, a, b):
        k = owner(u, a, b)
        pltpu.make_async_copy(gathered.at[u, k], gathered.at[u, k], wide_recv.at[spot(u, a, b)]).wait()

    def slim(u, a, b, axis, way):
        k = owner(u, a, b)
        rows = pl.ds(32 * u, 32)
        return pltpu.make_async_remote_copy(
            src_ref=w_out.at[rows] if a == b == 0 else out_weights.at[k, rows],
            dst_ref=out_weights.at[k, rows],
            send_sem=out_send,
            recv_sem=out_recv.at[spot(u, *lands_at(u, a, b, axis, way))],
            device_id={axis: (here[axis] + way) % 4},
            device_id_type=MESH,
        )

    def slim_arrival(u, a, b):
        part = out_weights.at[owner(u, a, b), pl.ds(32 * u, 32)]
        pltpu.make_async_copy(part, part, out_recv.at[spot(u, a, b)]).wait()

    own, order = arrival_order()
    for u, axis, way in own:
        wide(u, 0, 0, axis, way).start()

    token_copy.wait()

    @pl.loop(0, 16)
    def _(i):
        rows = pl.ds(pl.multiple_of(16 * i, 16), 16)
        floated = raw[rows, :].astype(F32)
        scale = lax.rsqrt(jnp.mean(floated * floated, axis=-1, keepdims=True) + EPSILON)
        scaled = (floated * scale * gain[...]).astype(BF16)
        for k in range(16):
            normed[k, rows, :] = scaled[:, 256 * k : 256 * k + 256]

    def add_product(u, k, first=False):
        product = jnp.dot(normed[k], gathered[u, k], preferred_element_type=F32)
        sums[u] = product if first else sums[u] + product

    def pack_state(i):
        state_copy(i).wait()

        @pl.loop(0, 8)
        def _(j):
            packed[8 * i + j] = halves[i % 2, j].astype(BF16)

        if i + 2 < 8:
            state_copy(i + 2).start()

    for copy in own_copies:
        copy.wait()
    for u in range(4):
        add_product(u, mine, first=True)

    for n, (u, a, b) in enumerate(order):
        wide_arrival(u, a, b)
        for axis, way in forwards(u, a, b):
            wide(u, a, b, axis, way).start()
        if n == 47:
            for v, axis, way in own:
                slim(v, 0, 0, axis, way).start()
        add_product(u, owner(u, a, b))
        if n % 4 == 3 and n // 4 < 8:
            pack_state(n // 4)

    def slim_steps(at):
        for u, a, b in order[15 * at : 15 * at + 15]:
            slim_arrival(u, a, b)
            for axis, way in forwards(u, a, b):
                slim(u, a, b, axis, way).start()

    row = lax.broadcasted_iota(jnp.int32, (64, 128), 0)
    step = row % 4
    row16 = lax.broadcasted_iota(jnp.int32, (16, 128), 0)

    def head_copy(block, to):
        part = heads.at[me, pl.ds(64 * block, 64)]
        if to == 0:
            where, sem = {"c": 1 - c}, relay_recv.at[block]
        else:
            where, sem = {"x": (x + to) % 4}, head_recv.at[4 * to + block]
        return pltpu.make_async_remote_copy(
            src_ref=part, dst_ref=part, send_sem=head_send, recv_sem=sem,
            device_id=where, device_id_type=MESH,
        )

    for block in range(4):
        rows = slice(64 * block, 64 * block + 64)
        for h in range(2):
            lanes = slice(128 * h, 128 * h + 128)
            q, p, v, gate = (
                sums[u, rows, lanes].astype(BF16).astype(F32) for u in range(4)
            )
            q = q * 128 ** -0.5
            g = gate_of(p, bound[:, lanes])
            k = 1.0 - g
            decay = g
            total = jnp.sum(q * k, axis=-1, keepdims=True) * v
            reach = jnp.where(step == 0, g, 0.0)
            for lag in (1, 2, 3):
                score = jnp.sum(q * decay * pltpu.roll(k, lag, 0), axis=-1, keepdims=True)
                total = total + jnp.where(step >= lag, score * pltpu.roll(v, lag, 0), 0.0)
                decay = decay * pltpu.roll(g, lag, 0)
                reach = jnp.where(step == lag, decay, reach)
            queries[...] = (q * reach).astype(BF16)
            rest[...] = total
            for four in range(4):
                part = slice(16 * four, 16 * four + 16)
                lhs = queries[part]
                found = rest[part]
                for j in range(4):
                    seq = 16 * block + 4 * four + j
                    product = jnp.dot(lhs, packed[seq, h], preferred_element_type=F32)
                    found = found + jnp.where(row16 // 4 == j, product, 0.0)
                rest[part] = found
            total = rest[...]
            scaled = total * lax.rsqrt(jnp.mean(total * total, axis=-1, keepdims=True) + EPSILON)
            heads[me, rows, lanes] = (
                scaled * head_gain[:, lanes] * (gate * jax.nn.sigmoid(gate))
            ).astype(BF16)
        for to in (0, 1, 3, 2):
            head_copy(block, to).start()
        slim_steps(block)

    def relay(block, to, where):
        part = heads.at[(x - to) % 4 * 2 + where, pl.ds(64 * block, 64)]
        return pltpu.make_async_remote_copy(
            src_ref=part, dst_ref=part, send_sem=head_send, recv_sem=relay_recv.at[4 * to + block],
            device_id={"c": 1 - c}, device_id_type=MESH,
        )

    for block in range(4):
        for to in (1, 3, 2):
            part = heads.at[(x - to) % 4 * 2 + c, pl.ds(64 * block, 64)]
            pltpu.make_async_copy(part, part, head_recv.at[4 * to + block]).wait()
            relay(block, to, c).start()
    for to in (0, 1, 3, 2):
        for block in range(4):
            relay(block, to, 1 - c).wait_recv()

    for half in range(2):
        rows = slice(128 * half, 128 * half + 128)
        total = jnp.zeros((128, 512), F32)
        for t in range(8):
            weight = out_weights[2 * t : 2 * t + 2].reshape(256, 512)
            total = total + jnp.dot(heads[t, rows], weight, preferred_element_type=F32)
        mixed[rows] = total.astype(BF16)

    sent = gathered.at[:, pl.ds(0, 15)]
    pltpu.make_async_copy(sent, sent, send_sem).wait()
    sent = out_weights.at[pl.ds(0, 15)]
    pltpu.make_async_copy(sent, sent, out_send).wait()
    sent = heads.at[pl.ds(0, 7)]
    pltpu.make_async_copy(sent, sent, head_send).wait()


def layer_of(tokens, gain, weights, bound, head_gain, w_out, taken):
    anywhere = pl.BlockSpec(memory_space=pl.ANY)
    inside = pl.BlockSpec(memory_space=pltpu.VMEM)
    return pl.pallas_call(
        layer_kernel,
        in_specs=[anywhere, inside] + [anywhere] * 4 + [inside, inside, anywhere, anywhere],
        out_specs=inside,
        out_shape=jax.ShapeDtypeStruct((256, 512), BF16),
        scratch_shapes=[
            pltpu.VMEM((256, 4096), BF16),
            pltpu.VMEM((16, 256, 256), BF16),
            pltpu.VMEM((4, 16, 256, 256), BF16),
            pltpu.VMEM((4, 256, 256), F32),
            pltpu.VMEM((16, 128, 512), BF16),
            pltpu.VMEM((2, 8, 2, 128, 128), F32),
            pltpu.VMEM((64, 2, 128, 128), BF16),
            pltpu.VMEM((8, 256, 256), BF16),
            pltpu.VMEM((64, 128), BF16),
            pltpu.VMEM((64, 128), F32),
            pltpu.SemaphoreType.DMA,
            pltpu.SemaphoreType.DMA((64,)),
            pltpu.SemaphoreType.DMA((64,)),
            pltpu.SemaphoreType.DMA,
            pltpu.SemaphoreType.DMA,
            pltpu.SemaphoreType.DMA((16,)),
            pltpu.SemaphoreType.DMA((16,)),
            pltpu.SemaphoreType.DMA((6,)),
            pltpu.SemaphoreType.DMA((2,)),
        ],
        compiler_params=pltpu.CompilerParams(collective_id=0, has_side_effects=True),
        name="layer",
    )(tokens, gain.reshape(1, 4096), *weights, bound.reshape(1, 256), head_gain.reshape(1, 256), w_out, taken)


def on_device(
    tokens, norm_gain, w_query, w_forget, w_value, w_gate, lower_bound, head_gain, w_out,
    state, prev_forget, prev_value, accepted,
):
    taken = taken_of(prev_forget, prev_value, lower_bound, accepted, state)
    mixed = layer_of(
        tokens, norm_gain, (w_query, w_forget, w_value, w_gate), lower_bound, head_gain, w_out, taken
    )
    return mixed, taken


def solution(mesh):
    finer = Mesh(mesh.devices.reshape(4, 4, 4, 2), ("z", "y", "x", "c"))
    kv, tp = ("z", "y"), ("x", "c")
    placed = (
        P(kv, None), P(), P(kv, tp), P(kv, tp), P(kv, tp), P(kv, tp), P(tp), P(tp), P(kv, tp),
        P(kv, tp, None, None), P(kv, None, tp), P(kv, None, tp), P(kv),
    )
    return jax.shard_map(
        on_device, mesh=finer, in_specs=placed,
        out_specs=(P(kv, tp), P(kv, tp, None, None)), check_vma=False,
    )
```

```python
import functools
import heapq

import jax
import jax.numpy as jnp
from jax import lax
from jax.experimental import pallas as pl
from jax.experimental.pallas import tpu as pltpu
from jax.sharding import Mesh
from jax.sharding import PartitionSpec as P

EPSILON = 1e-06
MESH = pl.DeviceIdType.MESH
F32, BF16 = jnp.float32, jnp.bfloat16

SIGN = ("z+", "z-", "z+", "z-")


def shifted(dz, link):
    return {"z+": (dz - 1) % 4, "z-": (dz + 1) % 4}.get(link, dz)


def sends(item):
    kind = item[0]
    if kind == "w":
        _, u, s, dz, dy = item
        way = SIGN[u]
        other = "z-" if way == "z+" else "z+"
        links = []
        if u < 2:
            if dy == 0:
                if dz == 0:
                    links = [way, other]
                elif dz == (3 if way == "z+" else 1):
                    links = [way]
                links = links + ["yi"]
        else:
            if dz == 0:
                links = (["yi"] if dy == 0 else []) + [way, other]
            elif dz == (3 if way == "z+" else 1):
                links = [way]
        return [(k, ("w", u, s, shifted(dz, k), 1 if k == "yi" else dy)) for k in links]
    if kind == "o":
        _, u, dz, dy = item
        way = SIGN[u]
        other = "z-" if way == "z+" else "z+"
        along_y = {0: ["yi", "yo"], 1: ["yo"]}.get(dy, [])
        along_z = [way, other] if dz == 0 else [way] if dz == (3 if way == "z+" else 1) else []
        if u < 2:
            links = along_y + along_z if dz == 0 else along_z
        else:
            links = along_z + along_y if dy == 0 else along_y
        turned = {("yi", 0): 1, ("yo", 0): 3, ("yo", 1): 2}
        return [(k, ("o", u, shifted(dz, k), turned.get((k, dy), dy))) for k in links]
    if kind in "th":
        at, b = item[-2], item[-1]
        first, over = item[:-2], {"t": "u", "h": "g"}[kind]
        go = [("c", (over, *first[1:], at, b))]
        if at == 0:
            go = [("x+", (*first, 1, b)), ("x-", (*first, 2, b))] + go
        elif at == 1 and b % 2 == 0:
            go = [("x+", (*first, 3, b))] + go
        elif at == 2 and b % 2 == 1:
            go = [("x-", (*first, 3, b))] + go
        return go
    return []


SIZE = {"w": 64, "o": 32, "t": 128, "u": 128, "h": 16, "g": 16, "q": 64}
OUT_AT = 20
TIMES = {"norm": 2.2, "norm2": 2.2, "take": 1.4, "product": 0.17, "away": 0.15, "recur": 0.4}


@functools.cache
def plan():
    free, events, steps = {}, [], []
    now, count, arrived_w, out_started = 0.0, 0, 0, False
    done, ready = set(), []
    work = [("norm",)] + [("take", i) for i in range(8)]
    products = [(u, 0, 0, 0) for u in range(4)]
    stage = {"tokens": 0, "products": 0, "recur": 0}

    def send(item, link, there):
        nonlocal count
        begin = max(now, free.get(link, 0.0))
        rate = 0.0017 if link == "c" else 0.0215
        free[link] = begin + SIZE[item[0]] * rate
        count += 1
        heapq.heappush(events, (free[link] + (1.0 if link == "c" else 2.2), count, there))
        steps.append(("start", item, link, there))

    def go_on(item):
        for link, there in sends(item):
            send(item, link, there)

    own = [("w", u, 0, 0, 0) for u in range(4)]
    for u in (0, 2, 1, 3):
        send(("w", u, 1, None, None), "yo", ("w", u, 1, 0, 0))
        if u in (0, 1):
            send(("t", 0, u), "yo", ("t", 0, u))
    for item in own:
        go_on(item)

    def task():
        if work and work[0][0] == "norm":
            return work.pop(0)
        if stage["tokens"] == 16:
            stage["tokens"] = 0
            stage["ready"] = 1
            return ("norm2",)
        if "ready" in stage and products:
            stage["products"] += 1
            if stage["products"] == 64:
                work.extend([("away", b) for b in range(4)] + [("recur", 0, b) for b in range(4)])
            return ("product", *products.pop(0))
        return work.pop(0) if work else None

    while True:
        if events and events[0][0] <= now:
            _, _, item = heapq.heappop(events)
            steps.append(("wait", item))
            go_on(item)
            if item[0] == "w":
                products.append(item[1:])
                arrived_w += 1
                if arrived_w == OUT_AT:
                    for u in range(4):
                        go_on(("o", u, 0, 0))
            elif item[0] in "tu":
                stage["tokens"] += 1
            elif item[0] == "q":
                work.append(("recur", 1, item[1]))
            now += 0.02
            continue
        job = task()
        if job is not None:
            steps.append(job)
            now += TIMES[job[0]]
            if job[0] == "away":
                send(("q", job[1]), "yo", ("q", job[1]))
            elif job[0] == "recur":
                go_on(("h", job[1], 0, job[2]))
        elif events:
            now = events[0][0]
        else:
            return tuple(steps), now


def gate_of(pre_act, bound):
    return bound + (1.0 - bound) * jax.nn.sigmoid(pre_act)


def two_parts(x):
    high = x.astype(BF16).astype(F32)
    return high, x - high


def layer_kernel(
    accepted_in, tokens, gain_in, w0, w1, w2, w3, bound_in, head_gain_in, w_out, state, forget_in, value_in,
    taken, heads, out_weights,
    raw, raw_more, normed, gathered, sums, away, given, packed, queries, rest,
    gain, bound, head_gain, old_forget, old_value, accepted,
    send_sem, out_send, head_send, token_send, given_send,
    w_recv, o_recv, t_recv, h_recv, q_recv, local_sem, state_sem,
):
    z, y, x, c = (lax.axis_index(name) for name in ("z", "y", "x", "c"))
    inner, outer = y + 1 - 2 * (y % 2), 3 - y
    mine = z * 4 + y
    me = x * 2 + c
    head = y // 2
    weights = (w0, w1, w2, w3)
    target = {
        "z+": {"z": (z + 1) % 4}, "z-": {"z": (z + 3) % 4}, "yi": {"y": inner}, "yo": {"y": outer},
        "x+": {"x": (x + 1) % 4}, "x-": {"x": (x + 3) % 4}, "c": {"c": 1 - c},
    }

    barrier = pltpu.get_barrier_semaphore()
    for partner in target.values():
        pl.semaphore_signal(barrier, inc=1, device_id=partner, device_id_type=MESH)

    def columns(h):
        return pl.ds(pl.multiple_of(128 * h, 128), 128)

    token_copies = [
        pltpu.make_async_copy(tokens, raw, local_sem.at[0]),
        pltpu.make_async_copy(gain_in, gain, local_sem.at[1]),
    ]
    small_copies = [
        pltpu.make_async_copy(bound_in, bound, local_sem.at[2]),
        pltpu.make_async_copy(head_gain_in, head_gain, local_sem.at[3]),
        pltpu.make_async_copy(forget_in, old_forget, local_sem.at[4]),
        pltpu.make_async_copy(value_in, old_value, local_sem.at[5]),
        pltpu.make_async_copy(accepted_in, accepted, local_sem.at[11]),
    ]
    own_copies = [
        pltpu.make_async_copy(weights[u].at[:, columns(head)], gathered.at[u, mine], local_sem.at[6 + u])
        for u in range(4)
    ]
    own_copies.append(pltpu.make_async_copy(w_out, out_weights.at[mine], local_sem.at[10]))

    def state_copy(i):
        part = pl.ds(8 * i, 8)
        return pltpu.make_async_copy(state.at[part], taken.at[part], state_sem.at[i])

    for copy in token_copies + own_copies + small_copies:
        copy.start()
    for i in range(8):
        state_copy(i).start()
    pl.semaphore_wait(barrier, len(target))

    def chip(kind):
        return (x + (0, 3, 1, 2)[kind]) % 4

    def place(item, core):
        kind = item[0]
        if kind == "w":
            _, u, s, dz, dy = item
            row = y if dy == 0 else inner
            return gathered.at[u, (z + dz) % 4 * 4 + (3 - row if s else row)]
        if kind == "o":
            _, u, dz, dy = item
            row = (y, inner, (y + 2) % 4, outer)[dy]
            return out_weights.at[(z + dz) % 4 * 4 + row, pl.ds(32 * u, 32)]
        if kind in "tu":
            _, at, part = item
            return raw_more.at[chip(at) * 2 + core, pl.ds(16 * part, 16)]
        if kind in "hg":
            _, n, at, b = item
            which = (chip(at) * 2 + core) * 2 + (1 - head if n else head)
            return heads.at[which, pl.ds(64 * b, 64)]
        return given.at[item[1]]

    def arrival(item):
        kind = item[0]
        if kind == "w":
            _, u, s, dz, dy = item
            return w_recv.at[u * 16 + s * 8 + dz * 2 + dy]
        if kind == "o":
            _, u, dz, dy = item
            return o_recv.at[u * 16 + dz * 4 + dy]
        if kind in "tu":
            return t_recv.at[(8 if kind == "u" else 0) + item[1] * 2 + item[2]]
        if kind in "hg":
            _, n, at, b = item
            return h_recv.at[(32 if kind == "g" else 0) + n * 16 + at * 4 + b]
        return q_recv.at[item[1]]

    leaving = {"w": send_sem, "o": out_send, "t": token_send, "h": head_send, "q": given_send}

    def start(item, link, there):
        kind = item[0]
        if kind == "w" and item[3] is None:
            source, to = weights[item[1]].at[:, columns(1 - head)], gathered.at[item[1], mine]
        elif kind == "w" and item[2:] == (0, 0, 0):
            source, to = weights[item[1]].at[:, columns(head)], gathered.at[item[1], mine]
        elif kind == "o" and item[2:] == (0, 0):
            source, to = w_out.at[pl.ds(32 * item[1], 32)], place(item, c)
        elif kind == "t" and link == "yo":
            rows = pl.ds(pl.multiple_of(32 * me + 16 * item[2], 16), 16)
            source, to = tokens.at[rows], place(item, c)
        elif kind == "q":
            source, to = away.at[item[1]], given.at[item[1]]
        else:
            source = to = place(item, c)
        pltpu.make_async_remote_copy(
            src_ref=source, dst_ref=to, send_sem=leaving[kind], recv_sem=arrival(there),
            device_id=target[link], device_id_type=MESH,
        ).start()

    def wait(item):
        ref = place(item, 1 - c if item[0] in "ug" else c)
        pltpu.make_async_copy(ref, ref, arrival(item)).wait()

    def normalize(take_rows, first):
        @pl.loop(0, 16)
        def _(i):
            floated = take_rows(i).astype(F32)
            scale = lax.rsqrt(jnp.mean(floated * floated, axis=-1, keepdims=True) + EPSILON)
            scaled = (floated * scale * gain[...]).astype(BF16)
            rows = pl.ds(pl.multiple_of(first + 16 * i, 16), 16)
            for k in range(16):
                normed[k, rows, :] = scaled[:, 256 * k : 256 * k + 256]

    def norm():
        for copy in token_copies:
            copy.wait()
        normalize(lambda i: raw[pl.ds(pl.multiple_of(16 * i, 16), 16), :], 0)
        for copy in own_copies + small_copies:
            copy.wait()

    def norm2():
        normalize(lambda i: raw_more[i // 2, pl.ds(pl.multiple_of(i % 2 * 16, 16), 16), :], 256)

    begun = set()

    def product(u, s, dz, dy):
        row = y if dy == 0 else inner
        k = (z + dz) % 4 * 4 + (3 - row if s else row)
        found = jnp.dot(normed[k], gathered[u, k], preferred_element_type=F32)
        sums[u] = sums[u] + found if u in begun else found
        begun.add(u)

    row8 = lax.broadcasted_iota(jnp.int32, (8, 256), 0)
    row80 = lax.broadcasted_iota(jnp.int32, (80, 128), 0)

    def take(i):
        state_copy(i).wait()
        seqs = pl.ds(pl.multiple_of(8 * i, 8), 8)
        count = jnp.zeros((8, 256), jnp.int32)
        for j in range(8):
            count = jnp.where(row8 == j, accepted[8 * i + j], count)
        gates, keys = [], []
        for t in range(4):
            g = gate_of(old_forget[seqs, t, :].astype(F32), bound[...])
            gates.append(jnp.where(t < count, g, 1.0))
            keys.append(jnp.where(t < count, 1.0 - g, 0.0))
        after = jnp.ones_like(gates[0])
        parts = [None] * 4
        for t in (3, 2, 1, 0):
            parts[t] = two_parts(keys[t] * after)
            after = after * gates[t]
        left = jnp.concatenate([p[0] for p in parts] + [p[1] for p in parts] + list(two_parts(after)), axis=0)
        values = jnp.concatenate([old_value[seqs, t, :].astype(F32) for t in range(4)] * 2, axis=0)
        values = jnp.concatenate([values, jnp.zeros((16, 256), F32)], axis=0)
        for h in range(2):
            lanes = slice(128 * h, 128 * h + 128)
            right = []
            for j in range(8):
                own_rows = row80 % 8 == j
                right.append(jnp.where(own_rows, values[:, lanes], 0.0))
                right.append(jnp.where(own_rows & (row80 >= 64), 1.0, 0.0))
            both = lax.dot_general(
                left[:, lanes].astype(BF16), jnp.concatenate(right, axis=1).astype(BF16),
                (((0,), (0,)), ((), ())), preferred_element_type=F32,
            )
            for j in range(8):
                added = both[:, 256 * j : 256 * j + 128]
                decay = both[:, 256 * j + 128 : 256 * j + 256]
                after_j = taken[8 * i + j, h] * decay + added
                taken[8 * i + j, h] = after_j
                packed[8 * i + j, h] = after_j.astype(BF16)

    step = lax.broadcasted_iota(jnp.int32, (64, 128), 0) % 4
    row16 = lax.broadcasted_iota(jnp.int32, (16, 128), 0)

    def give(b):
        for u in range(4):
            away[b, u] = sums[u, 256 + 64 * b : 320 + 64 * b].astype(BF16)

    def recur(n, b):
        rows = slice(64 * b, 64 * b + 64)
        h = 1 - head if n else head
        parts = (given[b, u] if n else sums[u, rows].astype(BF16) for u in range(4))
        q, p, v, gate = (part.astype(F32) for part in parts)
        q = q * 128 ** -0.5
        g = gate_of(p, bound[:, columns(h)])
        k = 1.0 - g
        decay = g
        total = jnp.sum(q * k, axis=-1, keepdims=True) * v
        reach = jnp.where(step == 0, g, 0.0)
        for lag in (1, 2, 3):
            score = jnp.sum(q * decay * pltpu.roll(k, lag, 0), axis=-1, keepdims=True)
            total = total + jnp.where(step >= lag, score * pltpu.roll(v, lag, 0), 0.0)
            decay = decay * pltpu.roll(g, lag, 0)
            reach = jnp.where(step == lag, decay, reach)
        queries[...] = (q * reach).astype(BF16)
        rest[...] = total
        for four in range(4):
            part = slice(16 * four, 16 * four + 16)
            lhs = queries[part]
            found = rest[part]
            for j in range(4):
                product = jnp.dot(lhs, packed[16 * b + 4 * four + j, h], preferred_element_type=F32)
                found = found + jnp.where(row16 // 4 == j, product, 0.0)
            rest[part] = found
        total = rest[...]
        scaled = total * lax.rsqrt(jnp.mean(total * total, axis=-1, keepdims=True) + EPSILON)
        heads[2 * me + h, rows] = (
            scaled * head_gain[:, columns(h)] * (gate * jax.nn.sigmoid(gate))
        ).astype(BF16)

    run = {
        "start": start, "wait": wait, "norm": norm, "norm2": norm2, "take": take, "product": product,
        "away": give, "recur": recur,
    }
    for name, *details in plan()[0]:
        run[name](*details)

    for sent, sem in (
        (gathered.at[:, pl.ds(0, 15)], send_sem),
        (out_weights.at[pl.ds(0, 15)], out_send),
        (heads.at[pl.ds(0, 14)], head_send),
        (raw_more, token_send),
        (given, given_send),
    ):
        pltpu.make_async_copy(sent, sent, sem).wait()


def layer_of(*arrays):
    outside = pl.BlockSpec(memory_space=pltpu.HBM)
    return pl.pallas_call(
        layer_kernel,
        in_specs=[outside] * 13,
        out_specs=[pl.BlockSpec(memory_space=pltpu.VMEM)] * 3,
        out_shape=[
            pltpu.VMEM((64, 2, 128, 128), F32),
            pltpu.VMEM((16, 256, 128), BF16),
            pltpu.VMEM((16, 128, 512), BF16),
        ],
        scratch_shapes=[
            pltpu.VMEM((256, 4096), BF16),
            pltpu.VMEM((8, 32, 4096), BF16),
            pltpu.VMEM((16, 512, 256), BF16),
            pltpu.VMEM((4, 16, 256, 128), BF16),
            pltpu.VMEM((4, 512, 128), F32),
            pltpu.VMEM((4, 4, 64, 128), BF16),
            pltpu.VMEM((4, 4, 64, 128), BF16),
            pltpu.VMEM((64, 2, 128, 128), BF16),
            pltpu.VMEM((64, 128), BF16),
            pltpu.VMEM((64, 128), F32),
            pltpu.VMEM((1, 4096), F32),
            pltpu.VMEM((1, 256), F32),
            pltpu.VMEM((1, 256), F32),
            pltpu.VMEM((64, 4, 256), BF16),
            pltpu.VMEM((64, 4, 256), BF16),
            pltpu.SMEM((64,), jnp.int32),
            pltpu.SemaphoreType.DMA,
            pltpu.SemaphoreType.DMA,
            pltpu.SemaphoreType.DMA,
            pltpu.SemaphoreType.DMA,
            pltpu.SemaphoreType.DMA,
            pltpu.SemaphoreType.DMA((64,)),
            pltpu.SemaphoreType.DMA((64,)),
            pltpu.SemaphoreType.DMA((16,)),
            pltpu.SemaphoreType.DMA((64,)),
            pltpu.SemaphoreType.DMA((4,)),
            pltpu.SemaphoreType.DMA((12,)),
            pltpu.SemaphoreType.DMA((8,)),
        ],
        compiler_params=pltpu.CompilerParams(
            collective_id=0, has_side_effects=True, vmem_limit_bytes=36 * 2**20
        ),
        name="layer",
    )(*(pltpu.with_memory_space_constraint(a, pltpu.HBM) for a in arrays))


def finish_kernel(taken_in, heads, out_weights, mixed, taken, block, sems):
    copy = pltpu.make_async_copy(taken_in, taken, sems.at[0])
    copy.start()
    for half in range(2):
        rows = slice(128 * half, 128 * half + 128)
        total = jnp.zeros((128, 512), F32)
        for h in range(16):
            total = total + jnp.dot(heads[h, rows], out_weights[h], preferred_element_type=F32)
        block[rows] = total.astype(BF16)
    last = pltpu.make_async_copy(block, mixed, sems.at[1])
    last.start()
    copy.wait()
    last.wait()


def finish_of(taken, heads, out_weights):
    inside = pl.BlockSpec(memory_space=pltpu.VMEM)
    anywhere = pl.BlockSpec(memory_space=pl.ANY)
    return pl.pallas_call(
        finish_kernel,
        in_specs=[inside] * 3,
        out_specs=[anywhere] * 2,
        out_shape=[jax.ShapeDtypeStruct((256, 512), BF16), jax.ShapeDtypeStruct(taken.shape, F32)],
        scratch_shapes=[pltpu.VMEM((256, 512), BF16), pltpu.SemaphoreType.DMA((2,))],
        compiler_params=pltpu.CompilerParams(vmem_limit_bytes=8 * 2**20),
        name="finish",
    )(*(pltpu.with_memory_space_constraint(a, pltpu.VMEM) for a in (taken, heads, out_weights)))


def on_device(
    tokens, norm_gain, w_query, w_forget, w_value, w_gate, lower_bound, head_gain, w_out,
    state, prev_forget, prev_value, accepted,
):
    return finish_of(*layer_of(
        accepted, tokens, norm_gain.reshape(1, 4096), w_query, w_forget, w_value, w_gate,
        lower_bound.reshape(1, 256), head_gain.reshape(1, 256), w_out, state, prev_forget, prev_value,
    ))


def solution(mesh):
    finer = Mesh(mesh.devices.reshape(4, 4, 4, 2), ("z", "y", "x", "c"))
    kv, tp = ("z", "y"), ("x", "c")
    placed = (
        P(kv, None), P(), P(kv, tp), P(kv, tp), P(kv, tp), P(kv, tp), P(tp), P(tp), P(kv, tp),
        P(kv, tp, None, None), P(kv, None, tp), P(kv, None, tp), P(kv),
    )
    return jax.shard_map(
        on_device, mesh=finer, in_specs=placed,
        out_specs=(P(kv, tp), P(kv, tp, None, None)), check_vma=False,
    )
```

```python
import functools
import heapq

import jax
import jax.numpy as jnp
from jax import lax
from jax.experimental import pallas as pl
from jax.experimental.pallas import tpu as pltpu
from jax.sharding import Mesh
from jax.sharding import PartitionSpec as P

EPSILON = 1e-06
MESH = pl.DeviceIdType.MESH
F32, BF16 = jnp.float32, jnp.bfloat16

STAGES = ((0, 2), (1, 3))


def shifted(dz, link):
    return {"z+": (dz - 1) % 4, "z-": (dz + 1) % 4}.get(link, dz)


def sends(item):
    kind = item[0]
    if kind in "wo":
        _, u, s, dz, dy = item
        way, other = ("z+", "z-") if (u // 2 + s) % 2 == 0 else ("z-", "z+")
        along_z = [way, other] if dz == 0 else [way] if dz == (3 if way == "z+" else 1) else []
        if u < 2:
            links = along_z + ["yi"] if dy == 0 else []
        else:
            links = (["yi"] if dy == dz == 0 else []) + along_z
        return [(k, (kind, u, s, shifted(dz, k), 1 if k == "yi" else dy)) for k in links]
    if kind in "th":
        at, b = item[-2], item[-1]
        first, over = item[:-2], {"t": "u", "h": "g"}[kind]
        go = [("c", (over, *first[1:], at, b))]
        if at == 0:
            go = [("x+", (*first, 1, b)), ("x-", (*first, 2, b))] + go
        elif at == 1 and b % 2 == 0:
            go = [("x+", (*first, 3, b))] + go
        elif at == 2 and b % 2 == 1:
            go = [("x-", (*first, 3, b))] + go
        return go
    return []


SIZE = {"w": 64, "o": 32, "t": 128, "u": 128, "h": 16, "g": 16}
SECOND_AT, OUT_AT = 1, 60
FIRST_SENDS = (
    ("t", 0), ("t", 1), ("w", 0), ("w", 2), ("w", 1), ("w", 3), ("o", 0), ("o", 1), ("o", 2), ("o", 3),
)
TIMES = {"norm": 0.6, "norm2": 0.15, "take": 0.7, "product": 0.04, "away": 0.05, "recur": 0.4}


@functools.cache
def plan():
    free, events, steps, marks = {}, [], [], {}
    now, count, got = 0.0, 0, 0
    soon = [("norm", i) for i in range(4)]
    later = [("take", i, h) for i in range(8) for h in range(2)]
    products = {(stage, half): [] for stage in range(2) for half in range(2)}
    left = dict.fromkeys(products, 32)
    tokens = 16
    held = [("o", u, 0, 0, 0) for u in range(4)]
    returned = set()

    def send(item, link, there):
        nonlocal count
        begin = max(now, free.get(link, 0.0))
        size = (128 if item[1] == 0 else 32) if item[0] == "q" else SIZE[item[0]]
        free[link] = begin + size * (0.0017 if link == "c" else 0.0225)
        count += 1
        heapq.heappush(events, (free[link] + (1.0 if link == "c" else 2.2), count, there))
        steps.append(("start", item, link, there))

    def go_on(item):
        for link, there in sends(item):
            send(item, link, there)

    def swap(kind, u):
        send((kind, u, 1, None, None), "yo", (kind, u, 1, 0, 0))

    def add(u, *rest):
        for half in range(2):
            products[u % 2, half].append((half, u, *rest))

    def begin(which):
        for u in STAGES[which]:
            add(u, 0, 0, 0)
            go_on(("w", u, 0, 0, 0))

    def recur(n, b):
        soon.append(("recur", n, b))

    for step in FIRST_SENDS:
        if step[0] == "t":
            send(("t", 0, step[1]), "yo", ("t", 0, step[1]))
        else:
            swap(*step)
    begin(0)

    def task():
        for key in ((0, 0), (0, 1), (1, 0), (1, 1)):
            if products[key] and not (soon and soon[0][0] == "norm") and not (key[1] and tokens):
                left[key] -= 1
                job = ("product", *products[key].pop(0))
                if left[key] == 0 and key[1]:
                    soon[:0] = [("away", key[0], b) for b in range(4)]
                if key[0] and left[1, 0] == left[1, 1] == 0:
                    soon.extend(later)
                    later.clear()
                    for b in range(4):
                        recur(0, b)
                return job
            if soon and soon[0][0] in ("norm2", "away"):
                break
        if soon:
            return soon.pop(0)
        return later.pop(0) if later else None

    while True:
        if events and events[0][0] <= now:
            _, _, item = heapq.heappop(events)
            steps.append(("wait", item))
            now += 0.02
            if item[0] == "o" and item[2:] == (1, 0, 0) and held is not None:
                held.append(item)
                continue
            go_on(item)
            if item[0] == "w":
                add(*item[1:])
                got += 1
                if got == SECOND_AT:
                    begin(1)
                if got == OUT_AT:
                    for other in held:
                        go_on(other)
                    held = None
                if got == 60:
                    marks["weights"] = now
            elif item[0] in "tu":
                tokens -= 1
                steps.append(("norm2", item))
                now += TIMES["norm2"]
                if tokens == 0:
                    marks["tokens"] = now
            elif item[0] == "q":
                returned.add(item[1:])
                marks["q", *item[1:]] = now
                for b in range(4):
                    if (0, 0) in returned and (1, b) in returned:
                        returned.remove((1, b))
                        recur(1, b)
            elif item[0] == "o":
                marks["o"] = now
            continue
        job = task()
        if job is not None:
            steps.append(job)
            now += TIMES[job[0]]
            if job[0] == "away":
                if job[1] == 1:
                    send(("q", 1, job[2]), "yo", ("q", 1, job[2]))
                elif job[2] == 3:
                    send(("q", 0, 0), "yo", ("q", 0, 0))
            elif job[0] == "recur":
                go_on(("h", job[1], 0, job[2]))
                marks["recur"] = now
        elif events:
            now = events[0][0]
        else:
            marks["end"] = now
            return tuple(steps), now, marks


def gate_of(pre_act, bound):
    return bound + (1.0 - bound) * jax.nn.sigmoid(pre_act)


def two_parts(x):
    high = x.astype(BF16).astype(F32)
    return high, x - high


def layer_kernel(
    accepted_in, tokens, gain_in, w0, w1, w2, w3, bound_in, head_gain_in, w_out, state, forget_in, value_in,
    taken, heads, out_weights,
    raw, raw_more, normed, gathered, sums, away, given, packed, queries, rest,
    gain, bound, head_gain, old_forget, old_value, accepted,
    send_sem, out_send, head_send, token_send, given_send,
    w_recv, o_recv, t_recv, h_recv, q_recv, local_sem, state_sem,
):
    z, y, x, c = (lax.axis_index(name) for name in ("z", "y", "x", "c"))
    inner, outer = y + 1 - 2 * (y % 2), 3 - y
    mine = z * 4 + y
    me = x * 2 + c
    head = y // 2
    weights = (w0, w1, w2, w3)
    target = {
        "z+": {"z": (z + 1) % 4}, "z-": {"z": (z + 3) % 4}, "yi": {"y": inner}, "yo": {"y": outer},
        "x+": {"x": (x + 1) % 4}, "x-": {"x": (x + 3) % 4}, "c": {"c": 1 - c},
    }

    barrier = pltpu.get_barrier_semaphore()
    for partner in target.values():
        pl.semaphore_signal(barrier, inc=1, device_id=partner, device_id_type=MESH)

    def columns(h):
        return pl.ds(pl.multiple_of(128 * h, 128), 128)

    token_copies = [
        pltpu.make_async_copy(tokens, raw, local_sem.at[0]),
        pltpu.make_async_copy(gain_in, gain, local_sem.at[1]),
    ]
    small_copies = [
        pltpu.make_async_copy(bound_in, bound, local_sem.at[2]),
        pltpu.make_async_copy(head_gain_in, head_gain, local_sem.at[3]),
        pltpu.make_async_copy(forget_in, old_forget, local_sem.at[4]),
        pltpu.make_async_copy(value_in, old_value, local_sem.at[5]),
        pltpu.make_async_copy(accepted_in, accepted, local_sem.at[11]),
    ]
    own_copies = [
        pltpu.make_async_copy(weights[u].at[:, columns(head)], gathered.at[u, mine], local_sem.at[6 + u])
        for u in range(4)
    ]
    own_copies.append(pltpu.make_async_copy(w_out, out_weights.at[mine], local_sem.at[10]))

    def state_copy(i):
        part = pl.ds(8 * i, 8)
        return pltpu.make_async_copy(state.at[part], taken.at[part], state_sem.at[i])

    for copy in token_copies + own_copies + small_copies:
        copy.start()
    for i in range(8):
        state_copy(i).start()
    pl.semaphore_wait(barrier, len(target))

    def chip(kind):
        return (x + (0, 3, 1, 2)[kind]) % 4

    def place(item, core):
        kind = item[0]
        if kind in "wo":
            _, u, s, dz, dy = item
            row = y if dy == 0 else inner
            k = (z + dz) % 4 * 4 + (3 - row if s else row)
            return gathered.at[u, k] if kind == "w" else out_weights.at[k, pl.ds(32 * u, 32)]
        if kind in "tu":
            _, at, part = item
            return raw_more.at[chip(at) * 2 + core, pl.ds(16 * part, 16)]
        if kind in "hg":
            _, n, at, b = item
            which = (chip(at) * 2 + core) * 2 + (1 - head if n else head)
            return heads.at[which, pl.ds(64 * b, 64)]
        return given.at[0] if item[1] == 0 else given.at[1, item[2]]

    def arrival(item):
        kind = item[0]
        if kind in "wo":
            _, u, s, dz, dy = item
            return (w_recv if kind == "w" else o_recv).at[u * 16 + s * 8 + dz * 2 + dy]
        if kind in "tu":
            return t_recv.at[(8 if kind == "u" else 0) + item[1] * 2 + item[2]]
        if kind in "hg":
            _, n, at, b = item
            return h_recv.at[(32 if kind == "g" else 0) + n * 16 + at * 4 + b]
        return q_recv.at[item[1] * 4 + item[2]]

    leaving = {"w": send_sem, "o": out_send, "t": token_send, "h": head_send, "q": given_send}

    def start(item, link, there):
        kind = item[0]
        if kind == "w" and item[3] is None:
            source, to = weights[item[1]].at[:, columns(1 - head)], gathered.at[item[1], mine]
        elif kind == "w" and item[2:] == (0, 0, 0):
            source, to = weights[item[1]].at[:, columns(head)], gathered.at[item[1], mine]
        elif kind == "o" and (item[3] is None or item[2:] == (0, 0, 0)):
            rows = pl.ds(32 * item[1], 32)
            source, to = w_out.at[rows], out_weights.at[mine, rows]
        elif kind == "t" and link == "yo":
            rows = pl.ds(pl.multiple_of(32 * me + 16 * item[2], 16), 16)
            source, to = tokens.at[rows], place(item, c)
        elif kind == "q":
            to = place(item, c)
            source = away.at[0] if item[1] == 0 else away.at[1, item[2]]
        else:
            source = to = place(item, c)
        pltpu.make_async_remote_copy(
            src_ref=source, dst_ref=to, send_sem=leaving[kind], recv_sem=arrival(there),
            device_id=target[link], device_id_type=MESH,
        ).start()

    def wait(item):
        ref = place(item, 1 - c if item[0] in "ug" else c)
        pltpu.make_async_copy(ref, ref, arrival(item)).wait()

    def normalize(rows_in, first):
        floated = rows_in.astype(F32)
        scale = lax.rsqrt(jnp.mean(floated * floated, axis=-1, keepdims=True) + EPSILON)
        scaled = (floated * scale * gain[...]).astype(BF16)
        rows = pl.ds(pl.multiple_of(first, 16), 16)
        for k in range(16):
            normed[k, rows, :] = scaled[:, 256 * k : 256 * k + 256]

    def norm(quarter):
        if quarter == 0:
            for copy in token_copies:
                copy.wait()

        @pl.loop(4 * quarter, 4 * quarter + 4)
        def _(i):
            normalize(raw[pl.ds(pl.multiple_of(16 * i, 16), 16), :], 16 * i)

        if quarter == 3:
            for copy in own_copies + small_copies:
                copy.wait()

    def norm2(item):
        _, kind, part = item
        piece = chip(kind) * 2 + (1 - c if item[0] == "u" else c)
        normalize(raw_more[piece, 16 * part : 16 * part + 16, :], 256 + 32 * piece + 16 * part)

    begun = set()

    def product(half, u, s, dz, dy):
        row = y if dy == 0 else inner
        k = (z + dz) % 4 * 4 + (3 - row if s else row)
        rows = slice(256 * half, 256 * half + 256)
        found = jnp.dot(normed[k, rows], gathered[u, k], preferred_element_type=F32)
        sums[u, rows] = sums[u, rows] + found if (half, u) in begun else found
        begun.add((half, u))

    row8 = lax.broadcasted_iota(jnp.int32, (8, 128), 0)
    row80 = lax.broadcasted_iota(jnp.int32, (80, 128), 0)

    def take(i, h):
        if h == 0:
            state_copy(i).wait()
        lanes = slice(128 * h, 128 * h + 128)
        seqs = slice(8 * i, 8 * i + 8)
        count = jnp.zeros((8, 128), jnp.int32)
        for j in range(8):
            count = jnp.where(row8 == j, accepted[8 * i + j], count)
        gates, keys = [], []
        for t in range(4):
            g = gate_of(old_forget[seqs, t, lanes].astype(F32), bound[:, lanes])
            gates.append(jnp.where(t < count, g, 1.0))
            keys.append(jnp.where(t < count, 1.0 - g, 0.0))
        after = jnp.ones_like(gates[0])
        parts = [None] * 4
        for t in (3, 2, 1, 0):
            parts[t] = two_parts(keys[t] * after)
            after = after * gates[t]
        left = jnp.concatenate([p[0] for p in parts] + [p[1] for p in parts] + list(two_parts(after)), axis=0)
        values = [old_value[seqs, t, lanes].astype(F32) for t in range(4)] * 2
        values = jnp.concatenate(values + [jnp.zeros((16, 128), F32)], axis=0)
        right = []
        for j in range(8):
            own_rows = row80 % 8 == j
            right.append(jnp.where(own_rows, values, 0.0))
            right.append(jnp.where(own_rows & (row80 >= 64), 1.0, 0.0))
        both = lax.dot_general(
            left.astype(BF16), jnp.concatenate(right, axis=1).astype(BF16),
            (((0,), (0,)), ((), ())), preferred_element_type=F32,
        )
        for j in range(8):
            added = both[:, 256 * j : 256 * j + 128]
            decay = both[:, 256 * j + 128 : 256 * j + 256]
            after_j = taken[8 * i + j, h] * decay + added
            taken[8 * i + j, h] = after_j
            packed[8 * i + j, h] = after_j.astype(BF16)

    step = lax.broadcasted_iota(jnp.int32, (64, 128), 0) % 4
    row16 = lax.broadcasted_iota(jnp.int32, (16, 128), 0)

    def give(stage, b):
        for i, u in enumerate(STAGES[stage]):
            away[stage, b, i] = sums[u, 256 + 64 * b : 320 + 64 * b].astype(BF16)

    def recur(n, b):
        rows = slice(64 * b, 64 * b + 64)
        h = 1 - head if n else head
        parts = (given[u % 2, b, u // 2] if n else sums[u, rows].astype(BF16) for u in range(4))
        q, p, v, gate = (part.astype(F32) for part in parts)
        q = q * 128 ** -0.5
        g = gate_of(p, bound[:, columns(h)])
        k = 1.0 - g
        decay = g
        total = jnp.sum(q * k, axis=-1, keepdims=True) * v
        reach = jnp.where(step == 0, g, 0.0)
        for lag in (1, 2, 3):
            score = jnp.sum(q * decay * pltpu.roll(k, lag, 0), axis=-1, keepdims=True)
            total = total + jnp.where(step >= lag, score * pltpu.roll(v, lag, 0), 0.0)
            decay = decay * pltpu.roll(g, lag, 0)
            reach = jnp.where(step == lag, decay, reach)
        queries[...] = (q * reach).astype(BF16)
        rest[...] = total
        for four in range(4):
            part = slice(16 * four, 16 * four + 16)
            lhs = queries[part]
            found = rest[part]
            for j in range(4):
                product = jnp.dot(lhs, packed[16 * b + 4 * four + j, h], preferred_element_type=F32)
                found = found + jnp.where(row16 // 4 == j, product, 0.0)
            rest[part] = found
        total = rest[...]
        scaled = total * lax.rsqrt(jnp.mean(total * total, axis=-1, keepdims=True) + EPSILON)
        heads[2 * me + h, rows] = (
            scaled * head_gain[:, columns(h)] * (gate * jax.nn.sigmoid(gate))
        ).astype(BF16)

    run = {
        "start": start, "wait": wait, "norm": norm, "norm2": norm2, "take": take, "product": product,
        "away": give, "recur": recur,
    }
    for name, *details in plan()[0]:
        run[name](*details)

    for sent, sem in (
        (gathered.at[:, pl.ds(0, 15)], send_sem),
        (out_weights.at[pl.ds(0, 15)], out_send),
        (heads.at[pl.ds(0, 14)], head_send),
        (raw_more, token_send),
        (given, given_send),
    ):
        pltpu.make_async_copy(sent, sent, sem).wait()


def layer_of(*arrays):
    outside = pl.BlockSpec(memory_space=pltpu.HBM)
    return pl.pallas_call(
        layer_kernel,
        in_specs=[outside] * 13,
        out_specs=[pl.BlockSpec(memory_space=pltpu.VMEM)] * 3,
        out_shape=[
            pltpu.VMEM((64, 2, 128, 128), F32),
            pltpu.VMEM((16, 256, 128), BF16),
            pltpu.VMEM((16, 128, 512), BF16),
        ],
        scratch_shapes=[
            pltpu.VMEM((256, 4096), BF16),
            pltpu.VMEM((8, 32, 4096), BF16),
            pltpu.VMEM((16, 512, 256), BF16),
            pltpu.VMEM((4, 16, 256, 128), BF16),
            pltpu.VMEM((4, 512, 128), F32),
            pltpu.VMEM((2, 4, 2, 64, 128), BF16),
            pltpu.VMEM((2, 4, 2, 64, 128), BF16),
            pltpu.VMEM((64, 2, 128, 128), BF16),
            pltpu.VMEM((64, 128), BF16),
            pltpu.VMEM((64, 128), F32),
            pltpu.VMEM((1, 4096), F32),
            pltpu.VMEM((1, 256), F32),
            pltpu.VMEM((1, 256), F32),
            pltpu.VMEM((64, 4, 256), BF16),
            pltpu.VMEM((64, 4, 256), BF16),
            pltpu.SMEM((64,), jnp.int32),
            pltpu.SemaphoreType.DMA,
            pltpu.SemaphoreType.DMA,
            pltpu.SemaphoreType.DMA,
            pltpu.SemaphoreType.DMA,
            pltpu.SemaphoreType.DMA,
            pltpu.SemaphoreType.DMA((64,)),
            pltpu.SemaphoreType.DMA((64,)),
            pltpu.SemaphoreType.DMA((16,)),
            pltpu.SemaphoreType.DMA((64,)),
            pltpu.SemaphoreType.DMA((8,)),
            pltpu.SemaphoreType.DMA((12,)),
            pltpu.SemaphoreType.DMA((8,)),
        ],
        compiler_params=pltpu.CompilerParams(
            collective_id=0, has_side_effects=True, vmem_limit_bytes=36 * 2**20
        ),
        name="layer",
    )(*(pltpu.with_memory_space_constraint(a, pltpu.HBM) for a in arrays))


def finish_kernel(taken_in, heads, out_weights, mixed, taken, block, sems):
    copy = pltpu.make_async_copy(taken_in, taken, sems.at[0])
    copy.start()
    for half in range(2):
        rows = slice(128 * half, 128 * half + 128)
        total = jnp.zeros((128, 512), F32)
        for h in range(16):
            total = total + jnp.dot(heads[h, rows], out_weights[h], preferred_element_type=F32)
        block[rows] = total.astype(BF16)
    last = pltpu.make_async_copy(block, mixed, sems.at[1])
    last.start()
    copy.wait()
    last.wait()


def finish_of(taken, heads, out_weights):
    inside = pl.BlockSpec(memory_space=pltpu.VMEM)
    anywhere = pl.BlockSpec(memory_space=pl.ANY)
    return pl.pallas_call(
        finish_kernel,
        in_specs=[inside] * 3,
        out_specs=[anywhere] * 2,
        out_shape=[jax.ShapeDtypeStruct((256, 512), BF16), jax.ShapeDtypeStruct(taken.shape, F32)],
        scratch_shapes=[pltpu.VMEM((256, 512), BF16), pltpu.SemaphoreType.DMA((2,))],
        compiler_params=pltpu.CompilerParams(vmem_limit_bytes=8 * 2**20),
        name="finish",
    )(*(pltpu.with_memory_space_constraint(a, pltpu.VMEM) for a in (taken, heads, out_weights)))


def on_device(
    tokens, norm_gain, w_query, w_forget, w_value, w_gate, lower_bound, head_gain, w_out,
    state, prev_forget, prev_value, accepted,
):
    return finish_of(*layer_of(
        accepted, tokens, norm_gain.reshape(1, 4096), w_query, w_forget, w_value, w_gate,
        lower_bound.reshape(1, 256), head_gain.reshape(1, 256), w_out, state, prev_forget, prev_value,
    ))


def solution(mesh):
    finer = Mesh(mesh.devices.reshape(4, 4, 4, 2), ("z", "y", "x", "c"))
    kv, tp = ("z", "y"), ("x", "c")
    placed = (
        P(kv, None), P(), P(kv, tp), P(kv, tp), P(kv, tp), P(kv, tp), P(tp), P(tp), P(kv, tp),
        P(kv, tp, None, None), P(kv, None, tp), P(kv, None, tp), P(kv),
    )
    return jax.shard_map(
        on_device, mesh=finer, in_specs=placed,
        out_specs=(P(kv, tp), P(kv, tp, None, None)), check_vma=False,
    )
```

```python
import functools
import heapq

import jax
import jax.numpy as jnp
from jax import lax
from jax.experimental import pallas as pl
from jax.experimental.pallas import tpu as pltpu
from jax.sharding import Mesh
from jax.sharding import PartitionSpec as P

EPSILON = 1e-06
MESH = pl.DeviceIdType.MESH
F32, BF16 = jnp.float32, jnp.bfloat16

LAST = 3
DIRECT = (("h", 1),)
Z_FIRST, UP = (False, False, True, True, False, False, True, True), (False, True, True, False, True, True, False, False)
OUT_Z_FIRST, OUT_UP, OUT_BY_INNER = (False, False, True, True), (True, False, True, False), (False, False, True, False)


def shifted(dz, link):
    return {"z+": (dz - 1) % 4, "z-": (dz + 1) % 4}.get(link, dz)


def sends(item):
    kind = item[0]
    if kind == "o":
        _, u, dz, r = item
        way, other = ("z+", "z-") if OUT_UP[u] else ("z-", "z+")
        along_z = [way, other] if dz == 0 else [way] if dz == (3 if way == "z+" else 1) else []
        along_y = ["yo", "yi"] if r == 0 else []
        if r == (1 if OUT_BY_INNER[u] else 3):
            along_y = ["yo" if OUT_BY_INNER[u] else "yi"]
        if OUT_Z_FIRST[u]:
            links = along_z + along_y if r == 0 else along_y
        else:
            links = along_y + along_z if dz == 0 else along_z
        turned = {("yi", 0): 1, ("yo", 0): 3, ("yo", 1): 2, ("yi", 3): 2}
        return [(k, (kind, u, shifted(dz, k), turned.get((k, r), r))) for k in links]
    if kind == "w":
        _, u, s, dz, dy = item
        way, other = ("z+", "z-") if UP[2 * u + s] else ("z-", "z+")
        along_z = [way, other] if dz == 0 else [way] if dz == (3 if way == "z+" else 1) else []
        if Z_FIRST[2 * u + s]:
            links = along_z + ["yi"] if dy == 0 else []
        else:
            links = (["yi"] if dy == dz == 0 else []) + along_z
        return [(k, (kind, u, s, shifted(dz, k), 1 if k == "yi" else dy)) for k in links]
    if kind in "th":
        at, b = item[-2], item[-1]
        first, over = item[:-2], {"t": "u", "h": "g"}[kind]
        go = [("c", (over, *first[1:], at, b))]
        if at == 0:
            go = [("x+", (*first, 1, b)), ("x-", (*first, 2, b))] + go
        elif at == 1 and b % 2 == 0:
            go = [("x+", (*first, 3, b))] + ([("X+", (over, *first[1:], 3, b))] if first in DIRECT else []) + go
        elif at == 2 and b % 2 == 1:
            go = [("x-", (*first, 3, b))] + ([("X-", (over, *first[1:], 3, b))] if first in DIRECT else []) + go
        elif at == 3 and first in DIRECT:
            go = []
        return go
    return []


SIZE = {"w": 64, "o": 32, "t": 128, "u": 128, "h": 16, "g": 16}
SLACK = {"w": 0.6, "u": 1.0, "q": 0.5}
BEGIN_AT, EARLY_AT, OUT_AT = (0, 0, 0, 16), 16, (54, 54)
FIRST_SENDS = (("w", 1), ("t", 1), ("t", 0), ("w", 2), ("w", 0), ("w", 3))
TIMES = {"norm": 0.6, "norm2": 0.15, "take": 0.4, "product": 0.1, "away": 0.05, "recur": 0.4}


@functools.cache
def plan():
    free, events, steps, marks = {}, [], [], {}
    now, count, got = 0.0, 0, 0
    soon = [("norm", i) for i in range(4)]
    later = [("take", i, h) for i in range(8) for h in range(2)]
    products = [([], []) for _ in range(4)]
    left = [[16, 16] for _ in range(4)]
    tokens = 16
    held, shut = [], {"z+", "z-", "yi"}
    returned, ends = set(), []

    def send(item, link, there):
        nonlocal count
        lane = link.lower()
        begin = max(now, free.get(lane, 0.0))
        size = (16 if item[1] == LAST else 64) if item[0] == "q" else SIZE[item[0]]
        free[lane] = begin + size * (0.0017 if link == "c" else 0.0225)
        count += 1
        heapq.heappush(events, (free[lane] + (1.0 if link == "c" else 2.6), count, there))
        steps.append(("start", item, link, there))

    def go_on(item):
        for link, there in sends(item):
            if item[0] == "o" and link in shut:
                held.append((item, link, there))
            else:
                send(item, link, there)

    def add(u, *rest):
        for half in range(2):
            products[u][half].append((u, *rest))

    def begin():
        for u in range(4):
            if BEGIN_AT[u] == got:
                add(u, 0, 0, 0)
                go_on(("w", u, 0, 0, 0))

    def release(*links):
        shut.difference_update(links)
        for step in [step for step in held if step[1] in links]:
            held.remove(step)
            send(*step)

    def recur(n, b):
        soon.append(("recur", n, b))

    for step in FIRST_SENDS:
        if step[0] == "t":
            send(("t", 0, step[1]), "yo", ("t", 0, step[1]))
        else:
            send(("w", step[1], 1, None, None), "yo", ("w", step[1], 1, 0, 0))
    begin()

    def task():
        if soon and soon[0][0] in ("norm", "norm2", "away"):
            return soon.pop(0)
        for u in range(4):
            for half in range(2):
                if products[u][half] and not (half and tokens):
                    unit = products[u][half].pop(0)
                    if half == 0 and not tokens:
                        products[u][1].remove(unit)
                        half = 2
                    for one in range(2):
                        left[u][one] -= half in (one, 2)
                    if half and left[u][1] == 0:
                        soon[:0] = [("away", u, b) for b in range(4)]
                    if left[LAST] == [0, 0] or sum(map(sum, left)) == 0:
                        soon.extend(later)
                        later.clear()
                    if sum(map(sum, left)) == 0:
                        for b in range(4):
                            recur(0, b)
                    return ("product", half, *unit)
        if soon:
            return soon.pop(0)
        return later.pop(0) if later else None

    while True:
        if events and events[0][0] <= now:
            _, count_of, item = heapq.heappop(events)
            if count_of > 0 and not sends(item):
                if item[0] in "ogh":
                    ends.append(item)
                else:
                    heapq.heappush(events, (now + (0.0 if got > 50 else SLACK[item[0]]), -count_of, item))
                continue
            steps.append(("wait", item))
            now += 0.02
            go_on(item)
            if item[0] == "w":
                add(*item[1:])
                got += 1
                begin()
                if got == EARLY_AT:
                    for u in range(4):
                        go_on(("o", u, 0, 0))
                if got == OUT_AT[0]:
                    release("z+", "z-")
                if got == OUT_AT[1]:
                    release("yi")
                if got == 60:
                    marks["weights"] = now
            elif item[0] in "tu":
                tokens -= 1
                steps.append(("norm2", item))
                now += TIMES["norm2"]
                if tokens == 0:
                    marks["tokens"] = now
            elif item[0] == "q":
                returned.add(item[1:])
                marks["q", *item[1:]] = now
                for b in range(4):
                    if all((u, 0) in returned for u in range(4) if u != LAST) and (LAST, b) in returned:
                        returned.remove((LAST, b))
                        recur(1, b)
            elif item[0] == "o":
                marks["o"] = now
            continue
        job = task()
        if job is not None:
            steps.append(job)
            now += TIMES[job[0]]
            if job[0] == "away":
                if job[1] == LAST:
                    send(("q", LAST, job[2]), "yo", ("q", LAST, job[2]))
                elif job[2] == 3:
                    send(("q", job[1], 0), "yo", ("q", job[1], 0))
            elif job[0] == "recur":
                go_on(("h", job[1], 0, job[2]))
                marks["recur"] = now
        elif events:
            now = events[0][0]
        else:
            marks["end"] = now
            steps.extend(("wait", item) for item in ends)
            return tuple(steps), now, marks


def gate_of(pre_act, bound):
    return bound + (1.0 - bound) * jax.nn.sigmoid(pre_act)


def two_parts(x):
    high = x.astype(BF16).astype(F32)
    return high, x - high


def layer_kernel(
    accepted_in, tokens, gain_in, w0, w1, w2, w3, bound_in, head_gain_in, w_out, state, forget_in, value_in,
    taken, heads, out_weights,
    raw, raw_more, normed, gathered, sums, away, given, packed, queries, rest,
    gain, bound, head_gain, old_forget, old_value, accepted,
    send_sem, out_send, head_send, token_send, given_send,
    w_recv, o_recv, t_recv, h_recv, q_recv, local_sem, state_sem,
):
    z, y, x, c = (lax.axis_index(name) for name in ("z", "y", "x", "c"))
    inner, outer = y + 1 - 2 * (y % 2), 3 - y
    mine = z * 4 + y
    me = x * 2 + c
    head = y // 2
    weights = (w0, w1, w2, w3)
    target = {
        "z+": {"z": (z + 1) % 4}, "z-": {"z": (z + 3) % 4}, "yi": {"y": inner}, "yo": {"y": outer},
        "x+": {"x": (x + 1) % 4}, "x-": {"x": (x + 3) % 4}, "c": {"c": 1 - c},
        "X+": {"x": (x + 1) % 4, "c": 1 - c}, "X-": {"x": (x + 3) % 4, "c": 1 - c},
    }

    barrier = pltpu.get_barrier_semaphore()
    for partner in target.values():
        pl.semaphore_signal(barrier, inc=1, device_id=partner, device_id_type=MESH)

    def columns(h):
        return pl.ds(pl.multiple_of(128 * h, 128), 128)

    token_copies = [
        pltpu.make_async_copy(tokens, raw, local_sem.at[0]),
        pltpu.make_async_copy(gain_in, gain, local_sem.at[1]),
    ]
    small_copies = [
        pltpu.make_async_copy(bound_in, bound, local_sem.at[2]),
        pltpu.make_async_copy(head_gain_in, head_gain, local_sem.at[3]),
        pltpu.make_async_copy(forget_in, old_forget, local_sem.at[4]),
        pltpu.make_async_copy(value_in, old_value, local_sem.at[5]),
        pltpu.make_async_copy(accepted_in, accepted, local_sem.at[11]),
    ]
    own_copies = [
        pltpu.make_async_copy(weights[u].at[:, columns(head)], gathered.at[u, mine], local_sem.at[6 + u])
        for u in range(4)
    ]
    own_copies.append(pltpu.make_async_copy(w_out, out_weights.at[mine], local_sem.at[10]))

    def state_copy(i):
        part = pl.ds(8 * i, 8)
        return pltpu.make_async_copy(state.at[part], taken.at[part], state_sem.at[i])

    for copy in token_copies + own_copies + small_copies:
        copy.start()
    for i in range(8):
        state_copy(i).start()
    pl.semaphore_wait(barrier, len(target))

    def chip(kind):
        return (x + (0, 3, 1, 2)[kind]) % 4

    def place(item, core):
        kind = item[0]
        if kind == "w":
            _, u, s, dz, dy = item
            row = y if dy == 0 else inner
            return gathered.at[u, (z + dz) % 4 * 4 + (3 - row if s else row)]
        if kind == "o":
            _, u, dz, r = item
            row = (y, inner, (y + 2) % 4, outer)[r]
            return out_weights.at[(z + dz) % 4 * 4 + row, pl.ds(32 * u, 32)]
        if kind in "tu":
            _, at, part = item
            return raw_more.at[chip(at) * 2 + core, pl.ds(16 * part, 16)]
        if kind in "hg":
            _, n, at, b = item
            which = (chip(at) * 2 + core) * 2 + (1 - head if n else head)
            return heads.at[which, pl.ds(64 * b, 64)]
        return given.at[item[1], pl.ds(64 * item[2], 64)] if item[1] == LAST else given.at[item[1]]

    def arrival(item):
        kind = item[0]
        if kind == "w":
            _, u, s, dz, dy = item
            return w_recv.at[u * 16 + s * 8 + dz * 2 + dy]
        if kind == "o":
            _, u, dz, r = item
            return o_recv.at[u * 16 + dz * 4 + r]
        if kind in "tu":
            return t_recv.at[(8 if kind == "u" else 0) + item[1] * 2 + item[2]]
        if kind in "hg":
            _, n, at, b = item
            return h_recv.at[(32 if kind == "g" else 0) + n * 16 + at * 4 + b]
        return q_recv.at[item[1] * 4 + item[2]]

    leaving = {"w": send_sem, "o": out_send, "t": token_send, "h": head_send, "q": given_send}

    def start(item, link, there):
        kind = item[0]
        if kind == "w" and item[3] is None:
            source, to = weights[item[1]].at[:, columns(1 - head)], gathered.at[item[1], mine]
        elif kind == "w" and item[2:] == (0, 0, 0):
            source, to = weights[item[1]].at[:, columns(head)], gathered.at[item[1], mine]
        elif kind == "o" and item[2:] == (0, 0):
            source, to = w_out.at[pl.ds(32 * item[1], 32)], place(item, c)
        elif kind == "t" and link == "yo":
            rows = pl.ds(pl.multiple_of(32 * me + 16 * item[2], 16), 16)
            source, to = tokens.at[rows], place(item, c)
        elif kind == "q":
            to = place(item, c)
            source = away.at[item[1], pl.ds(64 * item[2], 64)] if item[1] == LAST else away.at[item[1]]
        else:
            source = to = place(item, c)
        pltpu.make_async_remote_copy(
            src_ref=source, dst_ref=to, send_sem=leaving[kind], recv_sem=arrival(there),
            device_id=target[link], device_id_type=MESH,
        ).start()

    def wait(item):
        ref = place(item, 1 - c if item[0] in "ug" else c)
        pltpu.make_async_copy(ref, ref, arrival(item)).wait()

    def normalize(rows_in, first):
        floated = rows_in.astype(F32)
        scale = lax.rsqrt(jnp.mean(floated * floated, axis=-1, keepdims=True) + EPSILON)
        scaled = (floated * scale * gain[...]).astype(BF16)
        rows = pl.ds(pl.multiple_of(first, 16), 16)
        for k in range(16):
            normed[k, rows, :] = scaled[:, 256 * k : 256 * k + 256]

    def norm(quarter):
        if quarter == 0:
            for copy in token_copies:
                copy.wait()

        @pl.loop(4 * quarter, 4 * quarter + 4)
        def _(i):
            normalize(raw[pl.ds(pl.multiple_of(16 * i, 16), 16), :], 16 * i)

        if quarter == 3:
            for copy in own_copies + small_copies:
                copy.wait()

    def norm2(item):
        _, kind, part = item
        piece = chip(kind) * 2 + (1 - c if item[0] == "u" else c)
        normalize(raw_more[piece, 16 * part : 16 * part + 16, :], 256 + 32 * piece + 16 * part)

    begun = set()

    def product(half, u, s, dz, dy):
        if half == 2 and ((0, u) in begun) != ((1, u) in begun):
            product(0, u, s, dz, dy)
            return product(1, u, s, dz, dy)
        row = y if dy == 0 else inner
        k = (z + dz) % 4 * 4 + (3 - row if s else row)
        rows = slice(0, 512) if half == 2 else slice(256 * half, 256 * half + 256)
        found = jnp.dot(normed[k, rows], gathered[u, k], preferred_element_type=F32)
        sums[u, rows] = sums[u, rows] + found if (half % 2, u) in begun else found
        begun.update((one, u) for one in range(2) if half in (one, 2))

    row8 = lax.broadcasted_iota(jnp.int32, (8, 128), 0)
    row80 = lax.broadcasted_iota(jnp.int32, (80, 128), 0)

    def take(i, h):
        if h == 0:
            state_copy(i).wait()
        lanes = slice(128 * h, 128 * h + 128)
        seqs = slice(8 * i, 8 * i + 8)
        count = jnp.zeros((8, 128), jnp.int32)
        for j in range(8):
            count = jnp.where(row8 == j, accepted[8 * i + j], count)
        gates, keys = [], []
        for t in range(4):
            g = gate_of(old_forget[seqs, t, lanes].astype(F32), bound[:, lanes])
            gates.append(jnp.where(t < count, g, 1.0))
            keys.append(jnp.where(t < count, 1.0 - g, 0.0))
        after = jnp.ones_like(gates[0])
        parts = [None] * 4
        for t in (3, 2, 1, 0):
            parts[t] = two_parts(keys[t] * after)
            after = after * gates[t]
        left = jnp.concatenate([p[0] for p in parts] + [p[1] for p in parts] + list(two_parts(after)), axis=0)
        values = [old_value[seqs, t, lanes].astype(F32) for t in range(4)] * 2
        values = jnp.concatenate(values + [jnp.zeros((16, 128), F32)], axis=0)
        right = []
        for j in range(8):
            own_rows = row80 % 8 == j
            right.append(jnp.where(own_rows, values, 0.0))
            right.append(jnp.where(own_rows & (row80 >= 64), 1.0, 0.0))
        both = lax.dot_general(
            left.astype(BF16), jnp.concatenate(right, axis=1).astype(BF16),
            (((0,), (0,)), ((), ())), preferred_element_type=F32,
        )
        for j in range(8):
            added = both[:, 256 * j : 256 * j + 128]
            decay = both[:, 256 * j + 128 : 256 * j + 256]
            after_j = taken[8 * i + j, h] * decay + added
            taken[8 * i + j, h] = after_j
            packed[8 * i + j, h] = after_j.astype(BF16)

    step = lax.broadcasted_iota(jnp.int32, (64, 128), 0) % 4
    row16 = lax.broadcasted_iota(jnp.int32, (16, 128), 0)

    def give(u, b):
        away[u, 64 * b : 64 * b + 64] = sums[u, 256 + 64 * b : 320 + 64 * b].astype(BF16)

    def recur(n, b):
        rows = slice(64 * b, 64 * b + 64)
        h = 1 - head if n else head
        parts = (given[u, rows] if n else sums[u, rows].astype(BF16) for u in range(4))
        q, p, v, gate = (part.astype(F32) for part in parts)
        q = q * 128 ** -0.5
        g = gate_of(p, bound[:, columns(h)])
        k = 1.0 - g
        decay = g
        total = jnp.sum(q * k, axis=-1, keepdims=True) * v
        reach = jnp.where(step == 0, g, 0.0)
        for lag in (1, 2, 3):
            score = jnp.sum(q * decay * pltpu.roll(k, lag, 0), axis=-1, keepdims=True)
            total = total + jnp.where(step >= lag, score * pltpu.roll(v, lag, 0), 0.0)
            decay = decay * pltpu.roll(g, lag, 0)
            reach = jnp.where(step == lag, decay, reach)
        queries[...] = (q * reach).astype(BF16)
        rest[...] = total
        for four in range(4):
            part = slice(16 * four, 16 * four + 16)
            lhs = queries[part]
            found = rest[part]
            for j in range(4):
                product = jnp.dot(lhs, packed[16 * b + 4 * four + j, h], preferred_element_type=F32)
                found = found + jnp.where(row16 // 4 == j, product, 0.0)
            rest[part] = found
        total = rest[...]
        scaled = total * lax.rsqrt(jnp.mean(total * total, axis=-1, keepdims=True) + EPSILON)
        heads[2 * me + h, rows] = (
            scaled * head_gain[:, columns(h)] * (gate * jax.nn.sigmoid(gate))
        ).astype(BF16)

    run = {
        "start": start, "wait": wait, "norm": norm, "norm2": norm2, "take": take, "product": product,
        "away": give, "recur": recur,
    }
    for name, *details in plan()[0]:
        run[name](*details)

    for sent, sem in (
        (gathered.at[:, pl.ds(0, 15)], send_sem),
        (out_weights.at[pl.ds(0, 15)], out_send),
        (heads.at[pl.ds(0, 14)], head_send),
        (raw_more, token_send),
        (given, given_send),
    ):
        pltpu.make_async_copy(sent, sent, sem).wait()


def layer_of(*arrays):
    outside = pl.BlockSpec(memory_space=pltpu.HBM)
    return pl.pallas_call(
        layer_kernel,
        in_specs=[outside] * 13,
        out_specs=[pl.BlockSpec(memory_space=pltpu.VMEM)] * 3,
        out_shape=[
            pltpu.VMEM((64, 2, 128, 128), F32),
            pltpu.VMEM((16, 256, 128), BF16),
            pltpu.VMEM((16, 128, 512), BF16),
        ],
        scratch_shapes=[
            pltpu.VMEM((256, 4096), BF16),
            pltpu.VMEM((8, 32, 4096), BF16),
            pltpu.VMEM((16, 512, 256), BF16),
            pltpu.VMEM((4, 16, 256, 128), BF16),
            pltpu.VMEM((4, 512, 128), F32),
            pltpu.VMEM((4, 256, 128), BF16),
            pltpu.VMEM((4, 256, 128), BF16),
            pltpu.VMEM((64, 2, 128, 128), BF16),
            pltpu.VMEM((64, 128), BF16),
            pltpu.VMEM((64, 128), F32),
            pltpu.VMEM((1, 4096), F32),
            pltpu.VMEM((1, 256), F32),
            pltpu.VMEM((1, 256), F32),
            pltpu.VMEM((64, 4, 256), BF16),
            pltpu.VMEM((64, 4, 256), BF16),
            pltpu.SMEM((64,), jnp.int32),
            pltpu.SemaphoreType.DMA,
            pltpu.SemaphoreType.DMA,
            pltpu.SemaphoreType.DMA,
            pltpu.SemaphoreType.DMA,
            pltpu.SemaphoreType.DMA,
            pltpu.SemaphoreType.DMA((64,)),
            pltpu.SemaphoreType.DMA((64,)),
            pltpu.SemaphoreType.DMA((16,)),
            pltpu.SemaphoreType.DMA((64,)),
            pltpu.SemaphoreType.DMA((16,)),
            pltpu.SemaphoreType.DMA((12,)),
            pltpu.SemaphoreType.DMA((8,)),
        ],
        compiler_params=pltpu.CompilerParams(
            collective_id=0, has_side_effects=True, vmem_limit_bytes=36 * 2**20
        ),
        name="layer",
    )(*(pltpu.with_memory_space_constraint(a, pltpu.HBM) for a in arrays))


def finish_kernel(taken_in, heads, out_weights, mixed, taken, block, sems):
    copy = pltpu.make_async_copy(taken_in, taken, sems.at[0])
    copy.start()
    for half in range(2):
        rows = slice(128 * half, 128 * half + 128)
        total = jnp.zeros((128, 512), F32)
        for h in range(16):
            total = total + jnp.dot(heads[h, rows], out_weights[h], preferred_element_type=F32)
        block[rows] = total.astype(BF16)
    last = pltpu.make_async_copy(block, mixed, sems.at[1])
    last.start()
    copy.wait()
    last.wait()


def finish_of(taken, heads, out_weights):
    inside = pl.BlockSpec(memory_space=pltpu.VMEM)
    anywhere = pl.BlockSpec(memory_space=pl.ANY)
    return pl.pallas_call(
        finish_kernel,
        in_specs=[inside] * 3,
        out_specs=[anywhere] * 2,
        out_shape=[jax.ShapeDtypeStruct((256, 512), BF16), jax.ShapeDtypeStruct(taken.shape, F32)],
        scratch_shapes=[pltpu.VMEM((256, 512), BF16), pltpu.SemaphoreType.DMA((2,))],
        compiler_params=pltpu.CompilerParams(vmem_limit_bytes=8 * 2**20),
        name="finish",
    )(*(pltpu.with_memory_space_constraint(a, pltpu.VMEM) for a in (taken, heads, out_weights)))


def on_device(
    tokens, norm_gain, w_query, w_forget, w_value, w_gate, lower_bound, head_gain, w_out,
    state, prev_forget, prev_value, accepted,
):
    return finish_of(*layer_of(
        accepted, tokens, norm_gain.reshape(1, 4096), w_query, w_forget, w_value, w_gate,
        lower_bound.reshape(1, 256), head_gain.reshape(1, 256), w_out, state, prev_forget, prev_value,
    ))


def solution(mesh):
    finer = Mesh(mesh.devices.reshape(4, 4, 4, 2), ("z", "y", "x", "c"))
    kv, tp = ("z", "y"), ("x", "c")
    placed = (
        P(kv, None), P(), P(kv, tp), P(kv, tp), P(kv, tp), P(kv, tp), P(tp), P(tp), P(kv, tp),
        P(kv, tp, None, None), P(kv, None, tp), P(kv, None, tp), P(kv),
    )
    return jax.shard_map(
        on_device, mesh=finer, in_specs=placed,
        out_specs=(P(kv, tp), P(kv, tp, None, None)), check_vma=False,
    )
```

```python
import functools
import heapq

import jax
import jax.numpy as jnp
from jax import lax
from jax.experimental import pallas as pl
from jax.experimental.pallas import tpu as pltpu
from jax.sharding import Mesh
from jax.sharding import PartitionSpec as P

EPSILON = 1e-06
MESH = pl.DeviceIdType.MESH
F32, BF16 = jnp.float32, jnp.bfloat16

LAST = 3
INNER_NOW = (False, True, True, False, True, True, False, False)
DIRECT = (("h", 1),)
Z_FIRST, UP = (False, False, True, True, False, False, True, True), (False, True, True, True, True, False, False, False)
OUT_Z_FIRST, OUT_UP, OUT_BY_INNER = (True, False, False, True), (False, False, True, False), (True, False, False, False)


def shifted(dz, link):
    return {"z+": (dz - 1) % 4, "z-": (dz + 1) % 4}.get(link, dz)


def sends(item):
    kind = item[0]
    if kind == "o":
        _, u, dz, r = item
        way, other = ("z+", "z-") if OUT_UP[u] else ("z-", "z+")
        along_z = [way, other] if dz == 0 else [way] if dz == (3 if way == "z+" else 1) else []
        along_y = ["yo", "yi"] if r == 0 else []
        if r == (1 if OUT_BY_INNER[u] else 3):
            along_y = ["yo" if OUT_BY_INNER[u] else "yi"]
        if OUT_Z_FIRST[u]:
            links = along_z + along_y if r == 0 else along_y
        else:
            links = along_y + along_z if dz == 0 else along_z
        turned = {("yi", 0): 1, ("yo", 0): 3, ("yo", 1): 2, ("yi", 3): 2}
        return [(k, (kind, u, shifted(dz, k), turned.get((k, r), r))) for k in links]
    if kind == "w":
        _, u, s, dz, dy = item
        way, other = ("z+", "z-") if UP[2 * u + s] else ("z-", "z+")
        along_z = [way, other] if dz == 0 else [way] if dz == (3 if way == "z+" else 1) else []
        if Z_FIRST[2 * u + s]:
            links = [] if dy else ["yi"] + along_z if INNER_NOW[2 * u + s] else along_z + ["yi"]
        else:
            links = (["yi"] if dy == dz == 0 else []) + along_z
        return [(k, (kind, u, s, shifted(dz, k), 1 if k == "yi" else dy)) for k in links]
    if kind in "th":
        at, b = item[-2], item[-1]
        first, over = item[:-2], {"t": "u", "h": "g"}[kind]
        go = [("c", (over, *first[1:], at, b))]
        if at == 0:
            go = [("x+", (*first, 1, b)), ("x-", (*first, 2, b))] + go
        elif at == 1 and b % 2 == 0:
            go = [("x+", (*first, 3, b))] + ([("X+", (over, *first[1:], 3, b))] if first in DIRECT else []) + go
        elif at == 2 and b % 2 == 1:
            go = [("x-", (*first, 3, b))] + ([("X-", (over, *first[1:], 3, b))] if first in DIRECT else []) + go
        elif at == 3 and first in DIRECT:
            go = []
        return go
    return []


SIZE = {"w": 64, "o": 32, "t": 128, "u": 128, "h": 16, "g": 16}
SLACK = {"w": 0.3, "u": 1.0, "q": 0.2}
BEGIN_AT, EARLY_AT, OUT_AT = (0, 0, 0, 8), 24, (50, 56, 54)
FIRST_SENDS = (("w", 1), ("t", 0), ("t", 1), ("w", 2), ("w", 0), ("w", 3))
TIMES = {"norm": 0.6, "norm2": 0.15, "take": 0.4, "product": 0.1, "away": 0.05, "recur": 0.4}


@functools.cache
def plan():
    free, events, steps, marks = {}, [], [], {}
    now, count, got = 0.0, 0, 0
    soon = [("norm", i) for i in range(4)]
    later = [("take", i, h) for i in range(8) for h in range(2)]
    products = [([], []) for _ in range(4)]
    left = [[16, 16] for _ in range(4)]
    tokens = 16
    held, shut = [], {"z", "first z", "yi"}

    def gate(item, link):
        return ("first z" if OUT_Z_FIRST[item[1]] else "z") if link[0] == "z" else link
    returned, ends = set(), []

    def send(item, link, there):
        nonlocal count
        lane = link.lower()
        begin = max(now, free.get(lane, 0.0))
        size = (16 if item[1] == LAST else 64) if item[0] == "q" else SIZE[item[0]]
        free[lane] = begin + size * (0.0017 if link == "c" else 0.0225)
        count += 1
        heapq.heappush(events, (free[lane] + (1.0 if link == "c" else 2.6), count, there))
        steps.append(("start", item, link, there))

    def go_on(item):
        for link, there in sends(item):
            if item[0] == "o" and gate(item, link) in shut:
                held.append((item, link, there))
            else:
                send(item, link, there)

    def add(u, *rest):
        for half in range(2):
            products[u][half].append((u, *rest))

    def begin():
        for u in range(4):
            if BEGIN_AT[u] == got:
                add(u, 0, 0, 0)
                go_on(("w", u, 0, 0, 0))

    def release(*links):
        shut.difference_update(links)
        for step in [step for step in held if gate(step[0], step[1]) in links]:
            held.remove(step)
            send(*step)

    def recur(n, b):
        soon.append(("recur", n, b))

    for step in FIRST_SENDS:
        if step[0] == "t":
            send(("t", 0, step[1]), "yo", ("t", 0, step[1]))
        else:
            send(("w", step[1], 1, None, None), "yo", ("w", step[1], 1, 0, 0))
    begin()

    def task():
        if soon and soon[0][0] in ("norm", "norm2", "away"):
            return soon.pop(0)
        for u in range(4):
            for half in range(2):
                if products[u][half] and not (half and tokens):
                    unit = products[u][half].pop(0)
                    if half == 0 and not tokens:
                        products[u][1].remove(unit)
                        half = 2
                    for one in range(2):
                        left[u][one] -= half in (one, 2)
                    if half and left[u][1] == 0:
                        soon[:0] = [("away", u, b) for b in range(4)]
                    if left[LAST] == [0, 0] or sum(map(sum, left)) == 0:
                        soon.extend(later)
                        later.clear()
                    if sum(map(sum, left)) == 0:
                        for b in range(4):
                            recur(0, b)
                    return ("product", half, *unit)
        if soon:
            return soon.pop(0)
        return later.pop(0) if later else None

    while True:
        if events and events[0][0] <= now:
            _, count_of, item = heapq.heappop(events)
            if count_of > 0 and not sends(item):
                if item[0] in "ogh":
                    ends.append(item)
                else:
                    heapq.heappush(events, (now + (0.0 if got > 50 else SLACK[item[0]]), -count_of, item))
                continue
            steps.append(("wait", item))
            now += 0.02
            go_on(item)
            if item[0] == "w":
                add(*item[1:])
                got += 1
                begin()
                if got == EARLY_AT:
                    for u in range(4):
                        go_on(("o", u, 0, 0))
                if got == OUT_AT[0]:
                    release("z")
                if got == OUT_AT[2]:
                    release("first z")
                if got == OUT_AT[1]:
                    release("yi")
                if got == 60:
                    marks["weights"] = now
            elif item[0] in "tu":
                tokens -= 1
                steps.append(("norm2", item))
                now += TIMES["norm2"]
                if tokens == 0:
                    marks["tokens"] = now
            elif item[0] == "q":
                returned.add(item[1:])
                marks["q", *item[1:]] = now
                for b in range(4):
                    if all((u, 0) in returned for u in range(4) if u != LAST) and (LAST, b) in returned:
                        returned.remove((LAST, b))
                        recur(1, b)
            elif item[0] == "o":
                marks["o"] = now
            continue
        job = task()
        if job is not None:
            steps.append(job)
            now += TIMES[job[0]]
            if job[0] == "away":
                if job[1] == LAST:
                    send(("q", LAST, job[2]), "yo", ("q", LAST, job[2]))
                elif job[2] == 3:
                    send(("q", job[1], 0), "yo", ("q", job[1], 0))
            elif job[0] == "recur":
                go_on(("h", job[1], 0, job[2]))
                marks["recur"] = now
        elif events:
            now = events[0][0]
        else:
            marks["end"] = now
            steps.extend(("wait", item) for item in ends)
            return tuple(steps), now, marks


def gate_of(pre_act, bound):
    return bound + (1.0 - bound) * jax.nn.sigmoid(pre_act)


def two_parts(x):
    high = x.astype(BF16).astype(F32)
    return high, x - high


def layer_kernel(
    accepted_in, tokens, gain_in, w0, w1, w2, w3, bound_in, head_gain_in, w_out, state, forget_in, value_in,
    taken, heads, out_weights,
    raw, raw_more, normed, gathered, sums, away, given, packed, queries, rest,
    gain, bound, head_gain, old_forget, old_value, accepted,
    send_sem, out_send, head_send, token_send, given_send,
    w_recv, o_recv, t_recv, h_recv, q_recv, local_sem, state_sem,
):
    z, y, x, c = (lax.axis_index(name) for name in ("z", "y", "x", "c"))
    inner, outer = y + 1 - 2 * (y % 2), 3 - y
    mine = z * 4 + y
    me = x * 2 + c
    head = y // 2
    weights = (w0, w1, w2, w3)
    target = {
        "z+": {"z": (z + 1) % 4}, "z-": {"z": (z + 3) % 4}, "yi": {"y": inner}, "yo": {"y": outer},
        "x+": {"x": (x + 1) % 4}, "x-": {"x": (x + 3) % 4}, "c": {"c": 1 - c},
        "X+": {"x": (x + 1) % 4, "c": 1 - c}, "X-": {"x": (x + 3) % 4, "c": 1 - c},
    }

    barrier = pltpu.get_barrier_semaphore()
    for partner in target.values():
        pl.semaphore_signal(barrier, inc=1, device_id=partner, device_id_type=MESH)

    def columns(h):
        return pl.ds(pl.multiple_of(128 * h, 128), 128)

    token_copies = [
        pltpu.make_async_copy(tokens, raw, local_sem.at[0]),
        pltpu.make_async_copy(gain_in, gain, local_sem.at[1]),
    ]
    small_copies = [
        pltpu.make_async_copy(bound_in, bound, local_sem.at[2]),
        pltpu.make_async_copy(head_gain_in, head_gain, local_sem.at[3]),
        pltpu.make_async_copy(forget_in, old_forget, local_sem.at[4]),
        pltpu.make_async_copy(value_in, old_value, local_sem.at[5]),
        pltpu.make_async_copy(accepted_in, accepted, local_sem.at[11]),
    ]
    own_copies = [
        pltpu.make_async_copy(weights[u].at[:, columns(head)], gathered.at[u, mine], local_sem.at[6 + u])
        for u in range(4)
    ]
    own_copies.append(pltpu.make_async_copy(w_out, out_weights.at[mine], local_sem.at[10]))

    def state_copy(i):
        part = pl.ds(8 * i, 8)
        return pltpu.make_async_copy(state.at[part], taken.at[part], state_sem.at[i])

    for copy in token_copies + own_copies + small_copies:
        copy.start()
    for i in range(8):
        state_copy(i).start()
    pl.semaphore_wait(barrier, len(target))

    def chip(kind):
        return (x + (0, 3, 1, 2)[kind]) % 4

    def place(item, core):
        kind = item[0]
        if kind == "w":
            _, u, s, dz, dy = item
            row = y if dy == 0 else inner
            return gathered.at[u, (z + dz) % 4 * 4 + (3 - row if s else row)]
        if kind == "o":
            _, u, dz, r = item
            row = (y, inner, (y + 2) % 4, outer)[r]
            return out_weights.at[(z + dz) % 4 * 4 + row, pl.ds(32 * u, 32)]
        if kind in "tu":
            _, at, part = item
            return raw_more.at[chip(at) * 2 + core, pl.ds(16 * part, 16)]
        if kind in "hg":
            _, n, at, b = item
            which = (chip(at) * 2 + core) * 2 + (1 - head if n else head)
            return heads.at[which, pl.ds(64 * b, 64)]
        return given.at[item[1], pl.ds(64 * item[2], 64)] if item[1] == LAST else given.at[item[1]]

    def arrival(item):
        kind = item[0]
        if kind == "w":
            _, u, s, dz, dy = item
            return w_recv.at[u * 16 + s * 8 + dz * 2 + dy]
        if kind == "o":
            _, u, dz, r = item
            return o_recv.at[u * 16 + dz * 4 + r]
        if kind in "tu":
            return t_recv.at[(8 if kind == "u" else 0) + item[1] * 2 + item[2]]
        if kind in "hg":
            _, n, at, b = item
            return h_recv.at[(32 if kind == "g" else 0) + n * 16 + at * 4 + b]
        return q_recv.at[item[1] * 4 + item[2]]

    leaving = {"w": send_sem, "o": out_send, "t": token_send, "h": head_send, "q": given_send}

    def start(item, link, there):
        kind = item[0]
        if kind == "w" and item[3] is None:
            source, to = weights[item[1]].at[:, columns(1 - head)], gathered.at[item[1], mine]
        elif kind == "w" and item[2:] == (0, 0, 0):
            source, to = weights[item[1]].at[:, columns(head)], gathered.at[item[1], mine]
        elif kind == "o" and item[2:] == (0, 0):
            source, to = w_out.at[pl.ds(32 * item[1], 32)], place(item, c)
        elif kind == "t" and link == "yo":
            rows = pl.ds(pl.multiple_of(32 * me + 16 * item[2], 16), 16)
            source, to = tokens.at[rows], place(item, c)
        elif kind == "q":
            to = place(item, c)
            source = away.at[item[1], pl.ds(64 * item[2], 64)] if item[1] == LAST else away.at[item[1]]
        else:
            source = to = place(item, c)
        pltpu.make_async_remote_copy(
            src_ref=source, dst_ref=to, send_sem=leaving[kind], recv_sem=arrival(there),
            device_id=target[link], device_id_type=MESH,
        ).start()

    def wait(item):
        ref = place(item, 1 - c if item[0] in "ug" else c)
        pltpu.make_async_copy(ref, ref, arrival(item)).wait()

    def normalize(rows_in, first):
        floated = rows_in.astype(F32)
        scale = lax.rsqrt(jnp.mean(floated * floated, axis=-1, keepdims=True) + EPSILON)
        scaled = (floated * scale * gain[...]).astype(BF16)
        rows = pl.ds(pl.multiple_of(first, 16), 16)
        for k in range(16):
            normed[k, rows, :] = scaled[:, 256 * k : 256 * k + 256]

    def norm(quarter):
        if quarter == 0:
            for copy in token_copies:
                copy.wait()

        @pl.loop(4 * quarter, 4 * quarter + 4)
        def _(i):
            normalize(raw[pl.ds(pl.multiple_of(16 * i, 16), 16), :], 16 * i)

        if quarter == 3:
            for copy in own_copies + small_copies:
                copy.wait()

    def norm2(item):
        _, kind, part = item
        piece = chip(kind) * 2 + (1 - c if item[0] == "u" else c)
        normalize(raw_more[piece, 16 * part : 16 * part + 16, :], 256 + 32 * piece + 16 * part)

    begun = set()

    def product(half, u, s, dz, dy):
        if half == 2 and ((0, u) in begun) != ((1, u) in begun):
            product(0, u, s, dz, dy)
            return product(1, u, s, dz, dy)
        row = y if dy == 0 else inner
        k = (z + dz) % 4 * 4 + (3 - row if s else row)
        rows = slice(0, 512) if half == 2 else slice(256 * half, 256 * half + 256)
        found = jnp.dot(normed[k, rows], gathered[u, k], preferred_element_type=F32)
        sums[u, rows] = sums[u, rows] + found if (half % 2, u) in begun else found
        begun.update((one, u) for one in range(2) if half in (one, 2))

    row8 = lax.broadcasted_iota(jnp.int32, (8, 128), 0)
    row80 = lax.broadcasted_iota(jnp.int32, (80, 128), 0)

    def take(i, h):
        if h == 0:
            state_copy(i).wait()
        lanes = slice(128 * h, 128 * h + 128)
        seqs = slice(8 * i, 8 * i + 8)
        count = jnp.zeros((8, 128), jnp.int32)
        for j in range(8):
            count = jnp.where(row8 == j, accepted[8 * i + j], count)
        gates, keys = [], []
        for t in range(4):
            g = gate_of(old_forget[seqs, t, lanes].astype(F32), bound[:, lanes])
            gates.append(jnp.where(t < count, g, 1.0))
            keys.append(jnp.where(t < count, 1.0 - g, 0.0))
        after = jnp.ones_like(gates[0])
        parts = [None] * 4
        for t in (3, 2, 1, 0):
            parts[t] = two_parts(keys[t] * after)
            after = after * gates[t]
        left = jnp.concatenate([p[0] for p in parts] + [p[1] for p in parts] + list(two_parts(after)), axis=0)
        values = [old_value[seqs, t, lanes].astype(F32) for t in range(4)] * 2
        values = jnp.concatenate(values + [jnp.zeros((16, 128), F32)], axis=0)
        right = []
        for j in range(8):
            own_rows = row80 % 8 == j
            right.append(jnp.where(own_rows, values, 0.0))
            right.append(jnp.where(own_rows & (row80 >= 64), 1.0, 0.0))
        both = lax.dot_general(
            left.astype(BF16), jnp.concatenate(right, axis=1).astype(BF16),
            (((0,), (0,)), ((), ())), preferred_element_type=F32,
        )
        for j in range(8):
            added = both[:, 256 * j : 256 * j + 128]
            decay = both[:, 256 * j + 128 : 256 * j + 256]
            after_j = taken[8 * i + j, h] * decay + added
            taken[8 * i + j, h] = after_j
            packed[8 * i + j, h] = after_j.astype(BF16)

    step = lax.broadcasted_iota(jnp.int32, (64, 128), 0) % 4
    row16 = lax.broadcasted_iota(jnp.int32, (16, 128), 0)

    def give(u, b):
        away[u, 64 * b : 64 * b + 64] = sums[u, 256 + 64 * b : 320 + 64 * b].astype(BF16)

    def recur(n, b):
        rows = slice(64 * b, 64 * b + 64)
        h = 1 - head if n else head
        parts = (given[u, rows] if n else sums[u, rows].astype(BF16) for u in range(4))
        q, p, v, gate = (part.astype(F32) for part in parts)
        q = q * 128 ** -0.5
        g = gate_of(p, bound[:, columns(h)])
        k = 1.0 - g
        decay = g
        total = jnp.sum(q * k, axis=-1, keepdims=True) * v
        reach = jnp.where(step == 0, g, 0.0)
        for lag in (1, 2, 3):
            score = jnp.sum(q * decay * pltpu.roll(k, lag, 0), axis=-1, keepdims=True)
            total = total + jnp.where(step >= lag, score * pltpu.roll(v, lag, 0), 0.0)
            decay = decay * pltpu.roll(g, lag, 0)
            reach = jnp.where(step == lag, decay, reach)
        queries[...] = (q * reach).astype(BF16)
        rest[...] = total
        for four in range(4):
            part = slice(16 * four, 16 * four + 16)
            lhs = queries[part]
            found = rest[part]
            for j in range(4):
                product = jnp.dot(lhs, packed[16 * b + 4 * four + j, h], preferred_element_type=F32)
                found = found + jnp.where(row16 // 4 == j, product, 0.0)
            rest[part] = found
        total = rest[...]
        scaled = total * lax.rsqrt(jnp.mean(total * total, axis=-1, keepdims=True) + EPSILON)
        heads[2 * me + h, rows] = (
            scaled * head_gain[:, columns(h)] * (gate * jax.nn.sigmoid(gate))
        ).astype(BF16)

    run = {
        "start": start, "wait": wait, "norm": norm, "norm2": norm2, "take": take, "product": product,
        "away": give, "recur": recur,
    }
    for name, *details in plan()[0]:
        run[name](*details)

    for sent, sem in (
        (gathered.at[:, pl.ds(0, 15)], send_sem),
        (out_weights.at[pl.ds(0, 15)], out_send),
        (heads.at[pl.ds(0, 14)], head_send),
        (raw_more, token_send),
        (given, given_send),
    ):
        pltpu.make_async_copy(sent, sent, sem).wait()


def layer_of(*arrays):
    outside = pl.BlockSpec(memory_space=pltpu.HBM)
    return pl.pallas_call(
        layer_kernel,
        in_specs=[outside] * 13,
        out_specs=[pl.BlockSpec(memory_space=pltpu.VMEM)] * 3,
        out_shape=[
            pltpu.VMEM((64, 2, 128, 128), F32),
            pltpu.VMEM((16, 256, 128), BF16),
            pltpu.VMEM((16, 128, 512), BF16),
        ],
        scratch_shapes=[
            pltpu.VMEM((256, 4096), BF16),
            pltpu.VMEM((8, 32, 4096), BF16),
            pltpu.VMEM((16, 512, 256), BF16),
            pltpu.VMEM((4, 16, 256, 128), BF16),
            pltpu.VMEM((4, 512, 128), F32),
            pltpu.VMEM((4, 256, 128), BF16),
            pltpu.VMEM((4, 256, 128), BF16),
            pltpu.VMEM((64, 2, 128, 128), BF16),
            pltpu.VMEM((64, 128), BF16),
            pltpu.VMEM((64, 128), F32),
            pltpu.VMEM((1, 4096), F32),
            pltpu.VMEM((1, 256), F32),
            pltpu.VMEM((1, 256), F32),
            pltpu.VMEM((64, 4, 256), BF16),
            pltpu.VMEM((64, 4, 256), BF16),
            pltpu.SMEM((64,), jnp.int32),
            pltpu.SemaphoreType.DMA,
            pltpu.SemaphoreType.DMA,
            pltpu.SemaphoreType.DMA,
            pltpu.SemaphoreType.DMA,
            pltpu.SemaphoreType.DMA,
            pltpu.SemaphoreType.DMA((64,)),
            pltpu.SemaphoreType.DMA((64,)),
            pltpu.SemaphoreType.DMA((16,)),
            pltpu.SemaphoreType.DMA((64,)),
            pltpu.SemaphoreType.DMA((16,)),
            pltpu.SemaphoreType.DMA((12,)),
            pltpu.SemaphoreType.DMA((8,)),
        ],
        compiler_params=pltpu.CompilerParams(
            collective_id=0, has_side_effects=True, vmem_limit_bytes=36 * 2**20
        ),
        name="layer",
    )(*(pltpu.with_memory_space_constraint(a, pltpu.HBM) for a in arrays))


def finish_kernel(taken_in, heads, out_weights, mixed, taken, block, sems):
    copy = pltpu.make_async_copy(taken_in, taken, sems.at[0])
    copy.start()
    for half in range(2):
        rows = slice(128 * half, 128 * half + 128)
        total = jnp.zeros((128, 512), F32)
        for h in range(16):
            total = total + jnp.dot(heads[h, rows], out_weights[h], preferred_element_type=F32)
        block[rows] = total.astype(BF16)
    last = pltpu.make_async_copy(block, mixed, sems.at[1])
    last.start()
    copy.wait()
    last.wait()


def finish_of(taken, heads, out_weights):
    inside = pl.BlockSpec(memory_space=pltpu.VMEM)
    anywhere = pl.BlockSpec(memory_space=pl.ANY)
    return pl.pallas_call(
        finish_kernel,
        in_specs=[inside] * 3,
        out_specs=[anywhere] * 2,
        out_shape=[jax.ShapeDtypeStruct((256, 512), BF16), jax.ShapeDtypeStruct(taken.shape, F32)],
        scratch_shapes=[pltpu.VMEM((256, 512), BF16), pltpu.SemaphoreType.DMA((2,))],
        compiler_params=pltpu.CompilerParams(vmem_limit_bytes=8 * 2**20),
        name="finish",
    )(*(pltpu.with_memory_space_constraint(a, pltpu.VMEM) for a in (taken, heads, out_weights)))


def on_device(
    tokens, norm_gain, w_query, w_forget, w_value, w_gate, lower_bound, head_gain, w_out,
    state, prev_forget, prev_value, accepted,
):
    return finish_of(*layer_of(
        accepted, tokens, norm_gain.reshape(1, 4096), w_query, w_forget, w_value, w_gate,
        lower_bound.reshape(1, 256), head_gain.reshape(1, 256), w_out, state, prev_forget, prev_value,
    ))


def solution(mesh):
    finer = Mesh(mesh.devices.reshape(4, 4, 4, 2), ("z", "y", "x", "c"))
    kv, tp = ("z", "y"), ("x", "c")
    placed = (
        P(kv, None), P(), P(kv, tp), P(kv, tp), P(kv, tp), P(kv, tp), P(tp), P(tp), P(kv, tp),
        P(kv, tp, None, None), P(kv, None, tp), P(kv, None, tp), P(kv),
    )
    return jax.shard_map(
        on_device, mesh=finer, in_specs=placed,
        out_specs=(P(kv, tp), P(kv, tp, None, None)), check_vma=False,
    )
```
